32 devices in a mesh: ep: 4 (over z), tp: 8 (over y, x, core).
Axes of the slice: x: 2, y: 2, z: 4, core: 2. Of those that a mesh axis runs over, the one named last changes fastest.
Arguments:
- hidden_in: bfloat16 [48, 2048], P('ep', 'tp'), may hold values from -12 to 12
- state: float32 [48, 32, 128, 128], P('ep', 'tp'), may hold values from -3 to 3
- lower_bound: float32 [32, 128], P('tp'), may hold values from 0.05 to 0.95
- w_forget: bfloat16 [2048, 4096], P(None, 'tp'), may hold values from -0.125 to 0.125
- w_input: bfloat16 [2048, 4096], P(None, 'tp'), may hold values from -0.125 to 0.125
- w_query: bfloat16 [2048, 4096], P(None, 'tp'), may hold values from -0.125 to 0.125
- w_outgate: bfloat16 [2048, 4096], P(None, 'tp'), may hold values from -0.125 to 0.125
- head_gain: float32 [128], replicated, may hold values from 0.1 to 1.9
- w_out: bfloat16 [4096, 2048], P('tp'), may hold values from -0.125 to 0.125
- ln1_gain: float32 [2048], replicated, may hold values from 0.1 to 8
- ln1_bias: float32 [2048], replicated, may hold values from -1.5 to 1.5
- routes: int32 [48, 4], P('ep'), may hold values from 0 to 7, all different within a row; in each aligned block of 12 rows (0 to 11, 12 to 23, ...) at most 9 rows name the same one
- route_weights: float32 [48, 4], P('ep'), may hold values from 0.2 to 1.5
- exp_gate: bfloat16 [8, 2048, 4096], P('ep', None, 'tp'), may hold values from -0.125 to 0.125
- exp_up: bfloat16 [8, 2048, 4096], P('ep', None, 'tp'), may hold values from -0.125 to 0.125
- exp_down: bfloat16 [8, 4096, 2048], P('ep', 'tp'), may hold values from -0.125 to 0.125
- sh_gate: bfloat16 [2048, 512], P(None, 'tp'), may hold values from -0.125 to 0.125
- sh_up: bfloat16 [2048, 512], P(None, 'tp'), may hold values from -0.125 to 0.125
- sh_down: bfloat16 [512, 2048], P('tp'), may hold values from -0.25 to 0.25
- ln2_gain: float32 [2048], replicated, may hold values from 0.1 to 1.9
- ln2_bias: float32 [2048], replicated, may hold values from -1.5 to 1.5
Outputs:
- mixed_out: bfloat16 [48, 2048], P('ep', 'tp')
- new_state: float32 [48, 32, 128, 128], P('ep', 'tp')
The draws below stay inside these ranges and needn't reach their ends.
Inputs may be any that keep to these rules, and one draw needn't show every extreme that they name: `routes`: each row names 4 different experts; among the rows of one index of ep (12 rows) no expert is named more than 9 times, a bound that some block reaches.
All inputs are finite; a program needn't handle non-finite values.
Results may differ from the reference program's by a relative error of at most 0.023.
Values may be sent and summed in bfloat16 or wider, within the bound.
A program may use at most 64 MiB of HBM per device.

```python
import math
import jax
import jax.numpy as jnp
import numpy as np
from jax import lax

D = 2048
HEAD = 128
HEADS = 32
HD = 4096
EFF = 4096
SFF = 512
TOPK = 4
EXPERTS = 8
SEQ_DEV = 12
BATCH = 48
CAP = 9
N_EP = 4
N_TP = 8


def draw_hidden_in(key, part):
    first_key = jax.random.fold_in(jax.random.fold_in(key, 11), 0)
    ramp = jnp.exp(jnp.log(3.0) * jnp.arange(D, dtype=jnp.float32) / D)
    values = jnp.clip(jax.random.normal(first_key, (BATCH, D), jnp.float32), -4.0, 4.0) * ramp
    return values.astype(jnp.bfloat16)


def draw_ln1_gain(key, part):
    noise_key = jax.random.fold_in(key, 23)
    noise = jax.random.uniform(noise_key, (D,), jnp.float32, -1.0, 1.0)
    ramp = jnp.exp(jnp.log(3.0) * jnp.arange(D, dtype=jnp.float32) / D)
    return ((1.0 + 0.18 * noise) * ramp).astype(jnp.float32)


def strengthened(array, key, source, target, blocks, factor):
    owner, partner = [(jnp.arange(array.shape[axis_at]) // (array.shape[axis_at] // blocks)).reshape([-1 if axis == axis_at else 1 for axis in range(array.ndim)]) for axis_at in (source, target)]
    chosen = jax.random.permutation(key, blocks)[partner]
    strong = (owner == chosen) | (owner == (partner + blocks // 2) % blocks)
    return jnp.where(strong, factor * array, array)


def steps_of(key, shape, shards, low, high):
    level = 1.0
    for dim, blocks in shards:
        steps = jax.random.uniform(jax.random.fold_in(jax.random.fold_in(key, 6), dim), (blocks,), jnp.float32, low / len(shards), high / len(shards))
        level = level * jnp.repeat(jnp.exp(steps), shape[dim] // blocks).reshape((-1,) + (1,) * (len(shape) - 1 - dim))
    return level


def routed_block(own_key, own, number, rows, count, top, limit, skew):
    order = jax.random.permutation(own_key, count)
    heavy_load, ordinary = shares(count, rows * top, limit, skew, True), shares(count, rows * top, limit, skew, False)
    places = jnp.arange(count)

    def named(tallies, offset_by):
        used = int((tallies > 0).sum())
        fixed = max(1, used // 4)
        passed = fixed + (places - fixed + offset_by * (used - fixed)) % max(1, count - fixed)
        return jnp.zeros((count,), jnp.int32).at[order[jnp.where(places < fixed, places, passed)]].set(jnp.asarray(tallies, jnp.int32))

    tallies = jnp.where(number % 4 == 0, named(heavy_load, number // 4), named(ordinary, number - number // 4 - 1))
    mixed = jax.random.permutation(jax.random.fold_in(own, 3), count)
    donor, sink = mixed[0:count // 2 * 2:2], mixed[1:count // 2 * 2:2]
    slack = jnp.minimum(tallies[donor] - 1, limit - tallies[sink]) // 2
    slack = jnp.where((donor == order[0]) | (sink == order[0]) | (tallies[sink] == 0), 0, jnp.maximum(slack, 0))
    passed = jax.random.randint(jax.random.fold_in(own, 4), (count // 2,), 0, 1 << 20) % (slack + 1)
    tallies = tallies.at[donor].add(-passed).at[sink].add(passed)
    items = jnp.searchsorted(jnp.cumsum(tallies), jnp.arange(rows * top), side="right").astype(jnp.int32)
    table = items.reshape(top, rows).T
    table = table[jax.random.permutation(jax.random.fold_in(own, 1), rows)]
    offset_by = jax.random.randint(jax.random.fold_in(own, 2), (rows, 1), 0, top)
    return jnp.take_along_axis(table, (jnp.arange(top)[None, :] + offset_by) % top, axis=1)


def shares(number_of, total, limit, slope, full):
    weights = [(1 << 20) // math.isqrt(rank ** slope) + 1 for rank in range(1, number_of + 1)]
    largest = limit if full else min(limit, max(-(-total // number_of), total * weights[0] // sum(weights)))
    least = 1 if total - largest >= number_of - 1 else 0
    given, spare = [largest] + [least] * (number_of - 1), total - largest - least * (number_of - 1)
    while spare > 0:
        movable = [i for i in range(1, number_of) if given[i] < largest] or [i for i in range(1, number_of) if given[i] < limit]
        pool, left = sum([weights[i] for i in movable]), spare
        for i in movable:
            more = min(limit - given[i], max(1, left * weights[i] // pool), spare)
            given[i] = given[i] + more
            spare = spare - more
    return np.array(given)


def scatter_about(rng, dims, scale, most, pieces=(), kind=jnp.bfloat16):
    entries = scale * jax.random.normal(rng, dims, jnp.float32)
    if pieces:
        entries = entries * steps_of(rng, dims, pieces, -0.22, 0.18)
    return jnp.clip(entries, -most, most).astype(kind)


def bell_draw_with(stream_key, dims, deviation, limit, cuts, heavy, kind=jnp.bfloat16):
    values = deviation * jax.random.normal(stream_key, dims, jnp.float32)
    if cuts:
        values = values * steps_of(stream_key, dims, cuts, -0.22, 0.18)
    return jnp.clip(strengthened(values, jax.random.fold_in(stream_key, 3), *heavy), -limit, limit).astype(kind)


def setup_inputs(seed: int = 0) -> dict:
    keys = jax.random.split(jax.random.key(seed), 22)
    hidden_in = draw_hidden_in(jax.random.fold_in(keys[21], 71), 0)
    state = scatter_about(keys[1], (BATCH, HEADS, HEAD, HEAD), 0.5, 3.0, ((0, 4), (1, 8)), jnp.float32)
    lower_bound = jnp.clip(0.05 + 0.9 * jax.random.uniform(keys[2], (HEADS, HEAD), jnp.float32) ** steps_of(keys[2], (HEADS, HEAD), ((0, 8),), -0.2, 0.2), 0.05, 0.95)
    w_forget = scatter_about(keys[3], (D, HD), D ** -0.5, 0.125, ((1, 8),))
    w_input = scatter_about(keys[4], (D, HD), D ** -0.5, 0.125, ((1, 8),))
    w_query = scatter_about(keys[5], (D, HD), D ** -0.5, 0.125, ((1, 8),))
    w_outgate = scatter_about(keys[6], (D, HD), D ** -0.5, 0.125, ((1, 8),))
    head_gain = jnp.clip(1.0 + 0.18 * jax.random.normal(keys[7], (HEAD,), jnp.float32), 0.1, 1.9)
    w_out = bell_draw_with(keys[8], (HD, D), HD ** -0.5, 0.125, ((0, 8),), (0, 1, 8, 2.0))
    ln1_gain = draw_ln1_gain(jax.random.fold_in(keys[21], 71), 0)
    ln1_bias = scatter_about(keys[10], (D,), 0.3, 1.5, (), jnp.float32)
    routes_keys = jax.random.split(jax.random.fold_in(keys[11], 1), BATCH // SEQ_DEV)
    routes_turns = jax.random.permutation(jax.random.fold_in(keys[11], 3), BATCH // SEQ_DEV)
    routes = jax.vmap(lambda own, number: routed_block(jax.random.fold_in(keys[11], 2), own, number, SEQ_DEV, EXPERTS, TOPK, CAP, 2))(routes_keys, routes_turns).reshape((BATCH, TOPK))
    route_weights = jnp.clip(jnp.exp(math.log(1.5) - 2.014903 * jax.random.uniform(keys[12], (BATCH, TOPK), jnp.float32) ** steps_of(keys[12], (BATCH, TOPK), ((0, 4),), -0.2, 0.2)), 0.2, 1.5)
    exp_gate = scatter_about(keys[13], (EXPERTS, D, EFF), D ** -0.5, 0.125, ((0, 4), (2, 8)))
    exp_up = scatter_about(keys[14], (EXPERTS, D, EFF), D ** -0.5, 0.125, ((0, 4), (2, 8)))
    exp_down = bell_draw_with(keys[15], (EXPERTS, EFF, D), EFF ** -0.5, 0.125, ((0, 4), (1, 8)), (1, 2, 8, 2.0))
    sh_gate = scatter_about(keys[16], (D, SFF), D ** -0.5, 0.125, ((1, 8),))
    sh_up = scatter_about(keys[17], (D, SFF), D ** -0.5, 0.125, ((1, 8),))
    sh_down = scatter_about(keys[18], (SFF, D), SFF ** -0.5, 0.25, ((0, 8),))
    ln2_gain = jnp.clip(1.0 + 0.18 * jax.random.normal(keys[19], (D,), jnp.float32), 0.1, 1.9)
    ln2_bias = scatter_about(keys[20], (D,), 0.3, 1.5, (), jnp.float32)
    return {"hidden_in": hidden_in, "state": state, "lower_bound": lower_bound, "w_forget": w_forget, "w_input": w_input, "w_query": w_query, "w_outgate": w_outgate, "head_gain": head_gain, "w_out": w_out, "ln1_gain": ln1_gain, "ln1_bias": ln1_bias, "routes": routes, "route_weights": route_weights, "exp_gate": exp_gate, "exp_up": exp_up, "exp_down": exp_down, "sh_gate": sh_gate, "sh_up": sh_up, "sh_down": sh_down, "ln2_gain": ln2_gain, "ln2_bias": ln2_bias}


EPS = 1e-05
ALPHA = 2.0 ** 0.25

def rounded(value):
    return lax.optimization_barrier(value.astype(jnp.bfloat16)).astype(jnp.float32)

def layer_norm(value, gain, bias):
    average = lax.optimization_barrier(jnp.mean(value, -1, keepdims=True))
    centered = value - average
    variance = lax.optimization_barrier(jnp.mean(centered * centered, -1, keepdims=True))
    return centered * lax.rsqrt(variance + EPS) * gain + bias

def reference(hidden_in, state, lower_bound, w_forget, w_input, w_query, w_outgate, head_gain, w_out, ln1_gain, ln1_bias, routes, route_weights, exp_gate, exp_up, exp_down, sh_gate, sh_up, sh_down, ln2_gain, ln2_bias):

    def project(weight):
        return rounded(jnp.dot(hidden_in, weight, preferred_element_type=jnp.float32)).reshape(BATCH, HEADS, HEAD)
    forget_pre = project(w_forget)
    forget = lower_bound + (1.0 - lower_bound) * jax.nn.sigmoid(forget_pre)
    key_part = (1.0 - lower_bound) * jax.nn.sigmoid(-forget_pre)
    values = project(w_input)
    queries = jax.nn.silu(project(w_query))
    out_gate = jax.nn.silu(project(w_outgate))
    new_state = forget[..., None] * state + key_part[..., None] * values[:, :, None, :]
    readout = jnp.einsum('bhd,bhdv->bhv', queries, new_state, precision=lax.Precision.HIGHEST)
    normed = readout * lax.rsqrt(lax.optimization_barrier(jnp.mean(readout * readout, -1, keepdims=True)) + EPS) * head_gain
    mixed = (normed * out_gate).astype(jnp.bfloat16).reshape(BATCH, -1)
    branch = jnp.dot(mixed, w_out, preferred_element_type=jnp.float32)
    normed_rows = layer_norm(ALPHA * hidden_in.astype(jnp.float32) + branch, ln1_gain, ln1_bias).astype(jnp.bfloat16)
    shared_hidden = (jax.nn.silu(jnp.dot(normed_rows, sh_gate, preferred_element_type=jnp.float32)) * jnp.dot(normed_rows, sh_up, preferred_element_type=jnp.float32)).astype(jnp.bfloat16)
    shared_out = jnp.dot(shared_hidden, sh_down, preferred_element_type=jnp.float32)
    routes_flat = routes.reshape(N_EP, SEQ_DEV * TOPK).astype(jnp.int32)
    one_hot = (routes_flat[..., None] == jnp.arange(EXPERTS, dtype=jnp.int32)[None, None, :]).astype(jnp.int32)
    position = lax.optimization_barrier(jnp.sum((jnp.cumsum(one_hot, 1) - one_hot) * one_hot, -1)).astype(jnp.int32)
    group_index = jnp.arange(N_EP, dtype=jnp.int32)[:, None]
    slot_index = (routes_flat * (N_EP * CAP) + group_index * CAP + position).reshape(-1).astype(jnp.int32)
    token_index = group_index * SEQ_DEV + jnp.arange(SEQ_DEV * TOPK, dtype=jnp.int32)[None, :] // TOPK
    token_index = token_index.reshape(-1).astype(jnp.int32)
    buffer = jnp.zeros((EXPERTS * N_EP * CAP, D), jnp.bfloat16).at[slot_index].set(normed_rows[token_index])
    buffer = buffer.reshape(EXPERTS, N_EP * CAP, D)
    block_width = EFF // N_TP

    def run_expert(operands):
        block_rows, gate_weight, up_weight, down_weight = operands
        gate_part = jnp.dot(block_rows, gate_weight, preferred_element_type=jnp.float32)
        up_part = jnp.dot(block_rows, up_weight, preferred_element_type=jnp.float32)
        hidden_part = (jax.nn.silu(gate_part) * up_part).astype(jnp.bfloat16)
        hidden_blocks = hidden_part.reshape(-1, N_TP, block_width).astype(jnp.float32)
        down_blocks = down_weight.reshape(N_TP, block_width, D).astype(jnp.float32)
        parts = jnp.einsum('snf,nfd->nsd', hidden_blocks, down_blocks)
        return lax.optimization_barrier(jnp.sum(rounded(parts), 0))
    outputs = lax.map(run_expert, (buffer, exp_gate, exp_up, exp_down)).reshape(-1, D)
    picked = outputs[slot_index].reshape(BATCH, TOPK, D)
    routed = lax.optimization_barrier(jnp.sum(route_weights[..., None] * picked, 1))
    result = layer_norm(ALPHA * normed_rows.astype(jnp.float32) + routed + shared_out, ln2_gain, ln2_bias)
    return (result.astype(jnp.bfloat16), new_state)
```

```python
import functools

import jax
import jax.numpy as jnp
from jax import lax
from jax.experimental import pallas as pl
from jax.experimental.pallas import tpu as pltpu
from jax.sharding import PartitionSpec as P

EPS = 1e-05
ALPHA = 2.0**0.25
MESH = pl.DeviceIdType.MESH
F32 = jnp.float32
BF16 = jnp.bfloat16


def sigmoid(value):
    return jax.nn.sigmoid(value)


def silu(value):
    return value * jax.nn.sigmoid(value)


def dot(left, right):
    return jnp.dot(left, right, preferred_element_type=F32)


def layer_kernel(
    n_ep,
    n_tp,
    hid,
    lb,
    hg,
    g1,
    b1,
    routes,
    rw,
    g2,
    b2,
    state_h,
    wf_h,
    wi_h,
    wq_h,
    wo_h,
    wout_h,
    eg_h,
    eu_h,
    ed_h,
    sg_h,
    su_h,
    sd_h,
    out,
    ns_h,
    st,
    wf,
    wi,
    wq,
    wo,
    wout,
    eg,
    eu,
    ed,
    sg,
    su,
    sd,
    xf,
    xs,
    cws,
    cols_t,
    vals,
    ro,
    rs_send,
    rs,
    res,
    nr,
    cw_col,
    a2a_send,
    a2a,
    stat,
    load_sem,
    ns_sem,
    send_sem,
    recv_sem,
):
    n_all = n_ep * n_tp
    me_e = lax.axis_index("ep")
    me_t = lax.axis_index("tp")
    me = me_e * n_tp + me_t
    seqs = hid.shape[0]
    cols = hid.shape[1]
    rows = xf.shape[0]
    heads = lb.shape[0]
    head = lb.shape[1]
    local_experts = eg.shape[0]

    def device(index):
        return (index // n_tp, lax.rem(index, n_tp))

    first = [(wf_h, wf), (wi_h, wi), (wq_h, wq), (wo_h, wo), (state_h, st), (wout_h, wout)]
    second = [(eg_h, eg), (eu_h, eu), (sg_h, sg), (su_h, su), (ed_h, ed), (sd_h, sd)]
    loads = {}

    def start_loads(pairs, base):
        for i, (src, dst) in enumerate(pairs):
            loads[base + i] = pltpu.make_async_copy(src, dst, load_sem.at[base + i])
            loads[base + i].start()

    barrier = pltpu.get_barrier_semaphore()
    for k in range(1, n_all):
        pl.semaphore_signal(
            barrier, inc=1, device_id=device(lax.rem(me + k, n_all)), device_id_type=MESH
        )
    start_loads(first, 0)

    xf[...] = jnp.zeros_like(xf)
    xf[0:seqs, :] = hid[...].astype(F32)
    own_hidden = xf[...]
    xs[me_t] = own_hidden.astype(BF16)
    lanes = lax.broadcasted_iota(jnp.int32, (seqs, cws.shape[2]), 1)
    own_cw = jnp.zeros(lanes.shape, F32)
    for k in range(routes.shape[1]):
        own_cw += jnp.where(lanes == routes[:, k : k + 1], rw[:, k : k + 1], 0.0)
    cws[me_e] = jnp.zeros(cws.shape[1:], F32)
    cws[me_e, 0:seqs, :] = own_cw

    pl.semaphore_wait(barrier, n_all - 1)

    sends = []

    def send(src, dst, phase, target):
        copy = pltpu.make_async_remote_copy(
            src_ref=src,
            dst_ref=dst,
            send_sem=send_sem.at[phase],
            recv_sem=recv_sem.at[phase],
            device_id=target,
            device_id_type=MESH,
        )
        copy.start()
        sends.append(copy)

    def arrived(buffer, count, phase):
        part = buffer.at[pl.ds(0, count)]
        pltpu.make_async_copy(part, part, recv_sem.at[phase]).wait()

    for k in range(1, n_tp):
        send(xs.at[me_t], xs.at[me_t], 0, (me_e, lax.rem(me_t + k, n_tp)))
    for k in range(1, n_ep):
        send(cws.at[me_e], cws.at[me_e], 1, (lax.rem(me_e + k, n_ep), me_t))
    start_loads(second, len(first))

    arrived(xs, n_tp - 1, 0)
    x_full = jnp.concatenate([xs[t] for t in range(n_tp)], axis=1)

    def project(weight, index):
        loads[index].wait()
        return dot(x_full, weight[...]).astype(BF16).astype(F32)

    forget_pre = project(wf, 0)
    value_in = project(wi, 1)
    query = silu(project(wq, 2))
    out_gate = silu(project(wo, 3))
    for h in range(heads):
        span = slice(h * head, (h + 1) * head)
        bound = lb[h : h + 1, :]
        pre = forget_pre[:, span]
        forget = bound + (1.0 - bound) * sigmoid(pre)
        key = (1.0 - bound) * sigmoid(-pre)
        stacked = jnp.concatenate(
            [forget, key, query[:, span], jnp.zeros((head - 3 * rows, head), F32)], axis=0
        )
        cols_t[h] = stacked.T
        vals[h] = value_in[:, span]
    loads[4].wait()
    ro[...] = jnp.zeros_like(ro)
    outs = []
    for h in range(heads):
        for b in range(seqs):
            f_col = cols_t[h, :, b : b + 1]
            k_col = cols_t[h, :, rows + b : rows + b + 1]
            q_col = cols_t[h, :, 2 * rows + b : 2 * rows + b + 1]
            new = f_col * st[b, h] + k_col * vals[h, b : b + 1, :]
            st[b, h] = new
            ro[h, b : b + 1, :] = jnp.sum(q_col * new, axis=0, keepdims=True)
        outs.append(pltpu.make_async_copy(st.at[:, h], ns_h.at[:, h], ns_sem.at[h]))
        outs[-1].start()
    mixed = []
    for h in range(heads):
        readout = ro[h]
        scale = lax.rsqrt(jnp.mean(readout * readout, -1, keepdims=True) + EPS)
        gate = out_gate[:, h * head : (h + 1) * head]
        mixed.append((readout * scale * hg[...] * gate).astype(BF16))
    mixed = jnp.concatenate(mixed, axis=1)
    loads[5].wait()
    for t in range(n_tp):
        block = dot(mixed, wout[:, t * cols : (t + 1) * cols])
        rs_send[t] = block.astype(BF16)
    for k in range(1, n_tp):
        peer = lax.rem(me_t + k, n_tp)
        send(rs_send.at[peer], rs.at[me_t], 2, (me_e, peer))
    rs[me_t] = rs_send[me_t]
    arrived(rs, n_tp - 1, 2)
    total = ALPHA * own_hidden
    for t in range(n_tp):
        total += rs[t].astype(F32)
    res[me] = total.astype(BF16)
    for k in range(1, n_all):
        send(res.at[me], res.at[me], 3, device(lax.rem(me + k, n_all)))
    arrived(cws, n_ep - 1, 1)
    for g in range(n_ep):
        for j in range(local_experts):
            at = lax.broadcasted_iota(jnp.int32, cws.shape[1:], 1)
            cw_col[j, g * rows : (g + 1) * rows, :] = jnp.sum(
                jnp.where(at == me_e * local_experts + j, cws[g], 0.0), axis=1, keepdims=True
            )
    arrived(res, n_all - 1, 3)
    width = n_tp * cols
    for g in range(n_ep):
        row = jnp.concatenate([res[g * n_tp + t] for t in range(n_tp)], axis=1).astype(F32)
        centered = row - jnp.sum(row, -1, keepdims=True) / width
        variance = jnp.sum(centered * centered, -1, keepdims=True) / width
        normed = centered * lax.rsqrt(variance + EPS) * g1[...] + b1[...]
        nr[g * rows : (g + 1) * rows, :] = normed.astype(BF16)
    all_rows = nr[...]
    base = len(first)
    loads[base].wait()
    loads[base + 1].wait()
    hidden = []
    for j in range(local_experts):
        hidden.append((silu(dot(all_rows, eg[j])) * dot(all_rows, eu[j])).astype(BF16))
    loads[base + 2].wait()
    loads[base + 3].wait()
    own_rows = nr[pl.ds(pl.multiple_of(me_e * rows, rows), rows), :]
    shared = (silu(dot(own_rows, sg[...])) * dot(own_rows, su[...])).astype(BF16)
    loads[base + 4].wait()
    loads[base + 5].wait()
    weights = [cw_col[j] for j in range(local_experts)]
    for t in range(n_tp):
        span = slice(t * cols, (t + 1) * cols)
        acc = jnp.zeros((n_ep * rows, cols), F32)
        for j in range(local_experts):
            part = dot(hidden[j], ed[j, :, span]).astype(BF16).astype(F32)
            acc += weights[j] * part
        shared_part = dot(shared, sd[:, span])
        for g in range(n_ep):
            mine = jnp.where(me_e == g, 1.0, 0.0)
            block = acc[g * rows : (g + 1) * rows] + mine * shared_part
            a2a_send[g * n_tp + t] = block.astype(BF16)
    for k in range(1, n_all):
        peer = lax.rem(me + k, n_all)
        send(a2a_send.at[peer], a2a.at[me], 4, device(peer))
    a2a[me] = a2a_send[me]
    start = pl.multiple_of(me_t * cols, cols)
    own_cols = nr[pl.ds(pl.multiple_of(me_e * rows, rows), rows), pl.ds(start, cols)]
    final = ALPHA * own_cols.astype(F32)
    arrived(a2a, n_all - 1, 4)
    for i in range(n_all):
        final += a2a[i].astype(F32)
    mean_own = jnp.sum(final, -1, keepdims=True) / cols
    apart = final - mean_own
    spread_own = jnp.sum(apart * apart, -1, keepdims=True)
    lane = lax.broadcasted_iota(jnp.int32, stat.shape[1:], 1)
    stat[me_t] = jnp.where(lane == 0, mean_own, spread_own)
    for k in range(1, n_tp):
        send(stat.at[me_t], stat.at[me_t], 5, (me_e, lax.rem(me_t + k, n_tp)))
    gain = g2[:, pl.ds(start, cols)]
    bias = b2[:, pl.ds(start, cols)]
    arrived(stat, n_tp - 1, 5)
    means = [stat[t, :, 0:1] for t in range(n_tp)]
    mean = sum(means) / n_tp
    spread = jnp.zeros_like(mean)
    for t in range(n_tp):
        spread += stat[t, :, 1:2] + cols * (means[t] - mean) * (means[t] - mean)
    result = (final - mean) * lax.rsqrt(spread / width + EPS) * gain + bias
    out[...] = result[0:seqs, :].astype(BF16)
    for copy in sends:
        copy.wait_send()
    for copy in outs:
        copy.wait()


def fused(
    hidden_in,
    state,
    lower_bound,
    w_forget,
    w_input,
    w_query,
    w_outgate,
    head_gain,
    w_out,
    ln1_gain,
    ln1_bias,
    routes,
    route_weights,
    exp_gate,
    exp_up,
    exp_down,
    sh_gate,
    sh_up,
    sh_down,
    ln2_gain,
    ln2_bias,
):
    n_tp = lax.axis_size("tp")
    n_ep = lax.axis_size("ep")
    n_all = n_tp * n_ep
    seqs, cols = hidden_in.shape
    rows = -(-seqs // 16) * 16
    heads, head = lower_bound.shape
    local_experts = exp_gate.shape[0]
    whole = [
        state,
        w_forget,
        w_input,
        w_query,
        w_outgate,
        w_out,
        exp_gate,
        exp_up,
        exp_down,
        sh_gate,
        sh_up,
        sh_down,
    ]
    vmem = pl.BlockSpec(memory_space=pltpu.VMEM)
    hbm = pl.BlockSpec(memory_space=pltpu.HBM)
    scratch = [pltpu.VMEM(a.shape, a.dtype) for a in whole]
    scratch += [
        pltpu.VMEM((rows, cols), F32),
        pltpu.VMEM((n_tp, rows, cols), BF16),
        pltpu.VMEM((n_ep, rows, 128), F32),
        pltpu.VMEM((heads, head, head), F32),
        pltpu.VMEM((heads, rows, head), F32),
        pltpu.VMEM((heads, rows, head), F32),
        pltpu.VMEM((n_tp, rows, cols), BF16),
        pltpu.VMEM((n_tp, rows, cols), BF16),
        pltpu.VMEM((n_all, rows, cols), BF16),
        pltpu.VMEM((n_ep * rows, n_tp * cols), BF16),
        pltpu.VMEM((local_experts, n_ep * rows, 1), F32),
        pltpu.VMEM((n_all, rows, cols), BF16),
        pltpu.VMEM((n_all, rows, cols), BF16),
        pltpu.VMEM((n_tp, rows, 128), F32),
        pltpu.SemaphoreType.DMA((12,)),
        pltpu.SemaphoreType.DMA((heads,)),
        pltpu.SemaphoreType.DMA((6,)),
        pltpu.SemaphoreType.DMA((6,)),
    ]
    kernel = functools.partial(layer_kernel, n_ep, n_tp)
    row = lambda a: a.reshape(1, -1)
    mixed_out, new_state = pl.pallas_call(
        kernel,
        out_shape=(
            jax.ShapeDtypeStruct(hidden_in.shape, BF16),
            jax.ShapeDtypeStruct(state.shape, F32),
        ),
        in_specs=[vmem] * 9 + [hbm] * 12,
        out_specs=(vmem, hbm),
        scratch_shapes=scratch,
        compiler_params=pltpu.CompilerParams(
            collective_id=0, has_side_effects=True, vmem_limit_bytes=60 * 1024 * 1024
        ),
    )(
        hidden_in,
        lower_bound,
        row(head_gain),
        row(ln1_gain),
        row(ln1_bias),
        routes,
        route_weights,
        row(ln2_gain),
        row(ln2_bias),
        *whole,
    )
    return (mixed_out, new_state)


def fits(mesh, hidden_in, state, exp_gate):
    n_tp = mesh.shape["tp"]
    n_ep = mesh.shape["ep"]
    seqs = hidden_in.shape[0] // n_ep
    cols = hidden_in.shape[1] // n_tp
    weights = 3 * exp_gate.size * 2 // (n_tp * n_ep) + state.size * 4 // (n_tp * n_ep)
    return (
        cols % 128 == 0
        and seqs <= 16
        and state.shape[2] == 128
        and exp_gate.shape[0] <= 128
        and n_tp * n_ep <= 64
        and weights <= 24 * 1024 * 1024
    )


def rounded(value):
    return lax.optimization_barrier(value.astype(jnp.bfloat16)).astype(jnp.float32)


def local(
    hidden_in,
    state,
    lower_bound,
    w_forget,
    w_input,
    w_query,
    w_outgate,
    head_gain,
    w_out,
    ln1_gain,
    ln1_bias,
    routes,
    route_weights,
    exp_gate,
    exp_up,
    exp_down,
    sh_gate,
    sh_up,
    sh_down,
    ln2_gain,
    ln2_bias,
):
    n_tp = lax.axis_size("tp")
    n_ep = lax.axis_size("ep")
    seq_count = hidden_in.shape[0]
    col_count = hidden_in.shape[1]
    model_width = col_count * n_tp
    col_start = lax.axis_index("tp") * col_count
    heads_dev = state.shape[1]
    head_size = state.shape[2]
    top_count = routes.shape[1]
    local_experts = exp_gate.shape[0]
    expert_count = local_experts * n_ep
    capacity = max(2, 3 * seq_count * top_count // (2 * expert_count))
    slot_count = expert_count * capacity
    rows_full = lax.all_gather(hidden_in, "tp", axis=1, tiled=True)

    def project(weight):
        product = jnp.dot(rows_full, weight, preferred_element_type=jnp.float32)
        return rounded(product).reshape(seq_count, heads_dev, head_size)

    forget_pre = project(w_forget)
    forget = lower_bound + (1.0 - lower_bound) * jax.nn.sigmoid(forget_pre)
    key_part = (1.0 - lower_bound) * jax.nn.sigmoid(-forget_pre)
    values = project(w_input)
    queries = jax.nn.silu(project(w_query))
    out_gate = jax.nn.silu(project(w_outgate))
    new_state = forget[..., None] * state + key_part[..., None] * values[:, :, None, :]
    readout = jnp.einsum("bhd,bhdv->bhv", queries, new_state, precision=lax.Precision.HIGHEST)
    normed = readout * lax.rsqrt(jnp.mean(readout * readout, -1, keepdims=True) + EPS) * head_gain
    mixed = (normed * out_gate).astype(jnp.bfloat16).reshape(seq_count, heads_dev * head_size)
    branch = jnp.dot(mixed, w_out, preferred_element_type=jnp.float32)
    summed = lax.psum(branch.astype(jnp.bfloat16), "tp").astype(jnp.float32)
    residual = ALPHA * rows_full.astype(jnp.float32) + summed
    average = jnp.mean(residual, -1, keepdims=True)
    centered = residual - average
    variance = jnp.mean(centered * centered, -1, keepdims=True)
    normed_rows = (centered * lax.rsqrt(variance + EPS) * ln1_gain + ln1_bias).astype(jnp.bfloat16)
    routes_flat = routes.reshape(-1)
    one_hot = (routes_flat[:, None] == jnp.arange(expert_count, dtype=jnp.int32)[None, :]).astype(
        jnp.int32
    )
    position = jnp.sum((jnp.cumsum(one_hot, 0) - one_hot) * one_hot, 1)
    slot_index = routes_flat * capacity + position
    placing = (slot_index[:, None] == jnp.arange(slot_count, dtype=jnp.int32)[None, :]).astype(
        jnp.float32
    )
    chooser = jnp.sum(placing.reshape(seq_count, top_count, slot_count), 1).astype(jnp.bfloat16)
    weighted = jnp.sum(
        (placing * route_weights.reshape(-1)[:, None]).reshape(seq_count, top_count, slot_count), 1
    )
    own_cols = lax.dynamic_slice_in_dim(normed_rows, col_start, col_count, 1)
    picked = lax.dot_general(
        chooser, normed_rows, (((0,), (0,)), ((), ())), preferred_element_type=jnp.float32
    )
    arrived = lax.all_to_all(
        picked.astype(jnp.bfloat16).reshape(n_ep, local_experts * capacity, normed_rows.shape[1]),
        "ep",
        split_axis=0,
        concat_axis=0,
        tiled=True,
    )
    blocks = arrived.reshape(n_ep, local_experts, capacity, model_width)
    gate_part = jnp.einsum("gecd,edf->gecf", blocks, exp_gate, preferred_element_type=jnp.float32)
    up_part = jnp.einsum("gecd,edf->gecf", blocks, exp_up, preferred_element_type=jnp.float32)
    hidden_part = (jax.nn.silu(gate_part) * up_part).astype(jnp.bfloat16)
    expert_part = jnp.einsum(
        "gecf,efd->gecd", hidden_part, exp_down, preferred_element_type=jnp.float32
    )
    expert_part = expert_part.reshape(n_ep, local_experts * capacity, model_width).astype(
        jnp.bfloat16
    )
    shared_hidden = (
        jax.nn.silu(jnp.dot(normed_rows, sh_gate, preferred_element_type=jnp.float32))
        * jnp.dot(normed_rows, sh_up, preferred_element_type=jnp.float32)
    ).astype(jnp.bfloat16)
    shared_part = jnp.dot(shared_hidden, sh_down, preferred_element_type=jnp.float32)
    returned = lax.all_to_all(expert_part, "ep", split_axis=0, concat_axis=0, tiled=True)
    routed_partial = jnp.dot(
        weighted,
        returned.reshape(slot_count, model_width).astype(jnp.float32),
        precision=lax.Precision.HIGHEST,
    )
    combined = lax.psum_scatter(
        (routed_partial + shared_part).astype(jnp.bfloat16), "tp", scatter_dimension=1, tiled=True
    ).astype(jnp.float32)
    final_in = ALPHA * own_cols.astype(jnp.float32) + combined
    moments_two = lax.psum((jnp.sum(final_in, -1), jnp.sum(final_in * final_in, -1)), "tp")
    average_two = moments_two[0][:, None] / model_width
    variance_two = moments_two[1][:, None] / model_width - average_two * average_two
    gain_two = lax.dynamic_slice_in_dim(ln2_gain, col_start, col_count)
    bias_two = lax.dynamic_slice_in_dim(ln2_bias, col_start, col_count)
    mixed_out = (
        (final_in - average_two) * lax.rsqrt(variance_two + EPS) * gain_two + bias_two
    ).astype(jnp.bfloat16)
    return (mixed_out, new_state)


def solution(mesh):
    placed = (
        P("ep", "tp"),
        P("ep", "tp", None, None),
        P("tp", None),
        P(None, "tp"),
        P(None, "tp"),
        P(None, "tp"),
        P(None, "tp"),
        P(),
        P("tp", None),
        P(),
        P(),
        P("ep", None),
        P("ep", None),
        P("ep", None, "tp"),
        P("ep", None, "tp"),
        P("ep", "tp", None),
        P(None, "tp"),
        P(None, "tp"),
        P("tp", None),
        P(),
        P(),
    )

    def layer(*arrays):
        chosen = fused if fits(mesh, arrays[0], arrays[1], arrays[13]) else local
        return jax.shard_map(
            chosen,
            mesh=mesh,
            in_specs=placed,
            out_specs=(P("ep", "tp"), P("ep", "tp", None, None)),
            check_vma=False,
        )(*arrays)

    return layer
```

```python
import functools

import jax
import jax.numpy as jnp
from jax import lax
from jax.experimental import pallas as pl
from jax.experimental.pallas import tpu as pltpu
from jax.sharding import PartitionSpec as P

EPS = 1e-05
ALPHA = 2.0**0.25
MESH = pl.DeviceIdType.MESH
F32 = jnp.float32
BF16 = jnp.bfloat16


def sigmoid(value):
    return jax.nn.sigmoid(value)


def silu(value):
    return value * jax.nn.sigmoid(value)


def dot(left, right):
    return jnp.dot(left, right, preferred_element_type=F32)


def dot_t(left, right):
    dims = (((1,), (1,)), ((), ()))
    return lax.dot_general(left, right, dims, preferred_element_type=F32)


def layer_kernel(
    n_ep,
    n_tp,
    hid,
    lb,
    hg,
    g1,
    b1,
    routes,
    rw,
    g2,
    b2,
    state_h,
    wf_h,
    wi_h,
    wq_h,
    wo_h,
    wout_h,
    eg_h,
    eu_h,
    ed_h,
    sg_h,
    su_h,
    sd_h,
    out,
    ns_h,
    st,
    wf,
    wi,
    wq,
    wo,
    wout,
    eg,
    eu,
    ed,
    sg,
    su,
    sd,
    xf,
    xs,
    cws,
    cols_t,
    vals,
    ro,
    rs_send,
    rs,
    res,
    nr,
    cw_col,
    a2a_send,
    a2a,
    z_send,
    z_recv,
    acc_buf,
    cw_t,
    stat,
    load_sem,
    ns_sem,
    send_sem,
    recv_sem,
):
    me_e = lax.axis_index("ep")
    me_t = lax.axis_index("tp")
    seqs = hid.shape[0]
    cols = hid.shape[1]
    rows = xf.shape[0]
    heads = lb.shape[0]
    head = lb.shape[1]
    local_experts = eg.shape[0]

    first = [(wf_h, wf), (wi_h, wi), (wq_h, wq), (wo_h, wo), (state_h, st), (wout_h, wout)]
    second = [(eg_h, eg), (eu_h, eu), (sg_h, sg), (su_h, su), (ed_h, ed), (sd_h, sd)]
    loads = {}

    def start_loads(pairs, base):
        for i, (src, dst) in enumerate(pairs):
            loads[base + i] = pltpu.make_async_copy(src, dst, load_sem.at[base + i])
            loads[base + i].start()

    barrier = pltpu.get_barrier_semaphore()
    for k in range(1, n_ep):
        target = (lax.rem(me_e + k, n_ep), me_t)
        pl.semaphore_signal(barrier, inc=1, device_id=target, device_id_type=MESH)
    for k in range(1, n_tp):
        target = (me_e, lax.rem(me_t + k, n_tp))
        pl.semaphore_signal(barrier, inc=1, device_id=target, device_id_type=MESH)
    start_loads(first, 0)

    xf[...] = jnp.zeros_like(xf)
    xf[0:seqs, :] = hid[...].astype(F32)
    own_hidden = xf[...]
    xs[me_t] = own_hidden.astype(BF16)
    names = lax.broadcasted_iota(jnp.int32, (cw_t.shape[0], seqs), 0)
    own_cw = jnp.zeros(names.shape, F32)
    for k in range(routes.shape[0]):
        own_cw += jnp.where(names == routes[k : k + 1, :], rw[k : k + 1, :], 0.0)
    cw_t[...] = jnp.zeros_like(cw_t)
    cw_t[:, 0:seqs] = own_cw
    cws[me_e] = cw_t[...].T[0:rows, :]

    pl.semaphore_wait(barrier, n_ep + n_tp - 2)

    sends = []

    def send(src, dst, phase, target):
        copy = pltpu.make_async_remote_copy(
            src_ref=src,
            dst_ref=dst,
            send_sem=send_sem.at[phase],
            recv_sem=recv_sem.at[phase],
            device_id=target,
            device_id_type=MESH,
        )
        copy.start()
        sends.append(copy)

    def arrived(buffer, count, phase):
        part = buffer.at[pl.ds(0, count)]
        pltpu.make_async_copy(part, part, recv_sem.at[phase]).wait()

    for k in range(1, n_tp):
        send(xs.at[me_t], xs.at[me_t], 0, (me_e, lax.rem(me_t + k, n_tp)))
    for k in range(1, n_ep):
        send(cws.at[me_e], cws.at[me_e], 1, (lax.rem(me_e + k, n_ep), me_t))
    start_loads(second, len(first))

    arrived(xs, n_tp - 1, 0)
    x_full = jnp.concatenate([xs[t] for t in range(n_tp)], axis=1)

    def project(weight, index):
        loads[index].wait()
        return dot(x_full, weight[...]).astype(BF16).astype(F32)

    forget_pre = project(wf, 0)
    value_in = project(wi, 1)
    query = silu(project(wq, 2))
    out_gate = silu(project(wo, 3))
    for h in range(heads):
        span = slice(h * head, (h + 1) * head)
        bound = lb[h : h + 1, :]
        pre = forget_pre[:, span]
        forget = bound + (1.0 - bound) * sigmoid(pre)
        key = (1.0 - bound) * sigmoid(-pre)
        stacked = jnp.concatenate(
            [forget, key, query[:, span], jnp.zeros((head - 3 * rows, head), F32)], axis=0
        )
        cols_t[h] = stacked.T
        vals[h] = value_in[:, span]
    loads[4].wait()
    ro[...] = jnp.zeros_like(ro)
    outs = []
    for h in range(heads):
        for b in range(seqs):
            f_col = cols_t[h, :, b : b + 1]
            k_col = cols_t[h, :, rows + b : rows + b + 1]
            q_col = cols_t[h, :, 2 * rows + b : 2 * rows + b + 1]
            new = f_col * st[b, h] + k_col * vals[h, b : b + 1, :]
            st[b, h] = new
            ro[h, b : b + 1, :] = jnp.sum(q_col * new, axis=0, keepdims=True)
        outs.append(pltpu.make_async_copy(st.at[:, h], ns_h.at[:, h], ns_sem.at[h]))
        outs[-1].start()
    mixed = []
    for h in range(heads):
        readout = ro[h]
        scale = lax.rsqrt(jnp.mean(readout * readout, -1, keepdims=True) + EPS)
        gate = out_gate[:, h * head : (h + 1) * head]
        mixed.append((readout * scale * hg[...] * gate).astype(BF16))
    mixed = jnp.concatenate(mixed, axis=1)
    loads[5].wait()
    for k in list(range(1, n_tp)) + [0]:
        peer = lax.rem(me_t + k, n_tp)
        block = dot(mixed, wout[:, pl.ds(pl.multiple_of(peer * cols, cols), cols)])
        if k:
            rs_send[peer] = block.astype(BF16)
            send(rs_send.at[peer], rs.at[me_t], 2, (me_e, peer))
        else:
            rs[me_t] = block.astype(BF16)
    arrived(rs, n_tp - 1, 2)
    total = ALPHA * own_hidden
    for t in range(n_tp):
        total += rs[t].astype(F32)
    res[me_e, me_t] = total.astype(BF16)
    near = sorted(range(n_ep), key=lambda k: min(k, n_ep - k))
    for k in reversed(near[1:]):
        piece = res.at[me_e, me_t]
        send(piece, piece, 5 + k, (lax.rem(me_e + k, n_ep), me_t))
    width = n_tp * cols

    def forward(k):
        group = lax.rem(me_e + n_ep - k, n_ep)
        piece = res.at[group, me_t]
        if k:
            pltpu.make_async_copy(piece, piece, recv_sem.at[5 + k]).wait()
        for i in range(1, n_tp):
            send(piece, piece, 5 + n_ep + k, (me_e, lax.rem(me_t + i, n_tp)))

    def norm_group(k):
        group = lax.rem(me_e + n_ep - k, n_ep)
        arrived(res.at[group], n_tp - 1, 5 + n_ep + k)
        row = jnp.concatenate([res[group, t] for t in range(n_tp)], axis=1).astype(F32)
        centered = row - jnp.sum(row, -1, keepdims=True) / width
        variance = jnp.sum(centered * centered, -1, keepdims=True) / width
        normed = centered * lax.rsqrt(variance + EPS) * g1[...] + b1[...]
        nr[pl.ds(pl.multiple_of(group * rows, rows), rows), :] = normed.astype(BF16)

    forward(0)
    arrived(cws, n_ep - 1, 1)
    for g in range(n_ep):
        for j in range(local_experts):
            at = lax.broadcasted_iota(jnp.int32, cws.shape[1:], 1)
            cw_col[j, g * rows : (g + 1) * rows, :] = jnp.sum(
                jnp.where(at == me_e * local_experts + j, cws[g], 0.0), axis=1, keepdims=True
            )
    base = len(first)
    for k in near[1:]:
        forward(k)
    norm_group(0)
    own_rows = nr[pl.ds(pl.multiple_of(me_e * rows, rows), rows), :]
    loads[base + 2].wait()
    loads[base + 3].wait()
    shared = (silu(dot_t(own_rows, sg[...])) * dot_t(own_rows, su[...])).astype(BF16)
    for k in near[1:]:
        norm_group(k)
    all_rows = nr[...]
    loads[base].wait()
    loads[base + 1].wait()
    hidden = []
    for j in range(local_experts):
        hidden.append((silu(dot(all_rows, eg[j])) * dot(all_rows, eu[j])).astype(BF16))
    loads[base + 4].wait()
    loads[base + 5].wait()
    weights = [cw_col[j] for j in range(local_experts)]
    own_span = pl.ds(pl.multiple_of(me_e * rows, rows), rows)
    for k in list(range(1, n_tp)) + [0]:
        peer = lax.rem(me_t + k, n_tp)
        span = pl.ds(pl.multiple_of(peer * cols, cols), cols)
        acc = jnp.zeros((n_ep * rows, cols), F32)
        for j in range(local_experts):
            part = dot(hidden[j], ed[j, :, span]).astype(BF16).astype(F32)
            acc += weights[j] * part
        acc_buf[...] = acc
        acc_buf[own_span, :] += dot(shared, sd[:, span])
        if k:
            a2a_send[peer] = acc_buf[...].astype(BF16)
            send(a2a_send.at[peer], a2a.at[me_t], 4, (me_e, peer))
        else:
            a2a[me_t] = acc_buf[...].astype(BF16)
    start = pl.multiple_of(me_t * cols, cols)
    own_cols = nr[own_span, pl.ds(start, cols)]
    arrived(a2a, n_tp - 1, 4)
    plane = a2a[0].astype(F32)
    for i in range(1, n_tp):
        plane += a2a[i].astype(F32)
    acc_buf[...] = plane
    for g in range(n_ep):
        z_send[g] = plane[g * rows : (g + 1) * rows].astype(BF16)
    for k in range(1, n_ep):
        peer = lax.rem(me_e + k, n_ep)
        send(z_send.at[peer], z_recv.at[me_e], 3, (peer, me_t))
    z_recv[me_e] = z_send[me_e]
    final = ALPHA * own_cols.astype(F32)
    arrived(z_recv, n_ep - 1, 3)
    for g in range(n_ep):
        final += z_recv[g].astype(F32)
    mean_own = jnp.sum(final, -1, keepdims=True) / cols
    apart = final - mean_own
    spread_own = jnp.sum(apart * apart, -1, keepdims=True)
    lane = lax.broadcasted_iota(jnp.int32, stat.shape[1:], 1)
    stat[me_t] = jnp.where(lane == 0, mean_own, spread_own)
    for k in range(1, n_tp):
        send(stat.at[me_t], stat.at[me_t], 5, (me_e, lax.rem(me_t + k, n_tp)))
    gain = g2[:, pl.ds(start, cols)]
    bias = b2[:, pl.ds(start, cols)]
    arrived(stat, n_tp - 1, 5)
    means = [stat[t, :, 0:1] for t in range(n_tp)]
    mean = sum(means) / n_tp
    spread = jnp.zeros_like(mean)
    for t in range(n_tp):
        spread += stat[t, :, 1:2] + cols * (means[t] - mean) * (means[t] - mean)
    result = (final - mean) * lax.rsqrt(spread / width + EPS) * gain + bias
    out[...] = result[0:seqs, :].astype(BF16)
    for copy in sends:
        copy.wait_send()
    for copy in outs:
        copy.wait()


def fused(
    hidden_in,
    state,
    lower_bound,
    w_forget,
    w_input,
    w_query,
    w_outgate,
    head_gain,
    w_out,
    ln1_gain,
    ln1_bias,
    routes,
    route_weights,
    exp_gate,
    exp_up,
    exp_down,
    sh_gate,
    sh_up,
    sh_down,
    ln2_gain,
    ln2_bias,
):
    n_tp = lax.axis_size("tp")
    n_ep = lax.axis_size("ep")
    seqs, cols = hidden_in.shape
    rows = -(-seqs // 16) * 16
    heads, head = lower_bound.shape
    local_experts = exp_gate.shape[0]
    whole = [
        state,
        w_forget,
        w_input,
        w_query,
        w_outgate,
        w_out,
        exp_gate,
        exp_up,
        exp_down,
        sh_gate.T,
        sh_up.T,
        sh_down,
    ]
    vmem = pl.BlockSpec(memory_space=pltpu.VMEM)
    hbm = pl.BlockSpec(memory_space=pltpu.HBM)
    scratch = [pltpu.VMEM(a.shape, a.dtype) for a in whole]
    scratch += [
        pltpu.VMEM((rows, cols), F32),
        pltpu.VMEM((n_tp, rows, cols), BF16),
        pltpu.VMEM((n_ep, rows, 128), F32),
        pltpu.VMEM((heads, head, head), F32),
        pltpu.VMEM((heads, rows, head), F32),
        pltpu.VMEM((heads, rows, head), F32),
        pltpu.VMEM((n_tp, rows, cols), BF16),
        pltpu.VMEM((n_tp, rows, cols), BF16),
        pltpu.VMEM((n_ep, n_tp, rows, cols), BF16),
        pltpu.VMEM((n_ep * rows, n_tp * cols), BF16),
        pltpu.VMEM((local_experts, n_ep * rows, 1), F32),
        pltpu.VMEM((n_tp, n_ep * rows, cols), BF16),
        pltpu.VMEM((n_tp, n_ep * rows, cols), BF16),
        pltpu.VMEM((n_ep, rows, cols), BF16),
        pltpu.VMEM((n_ep, rows, cols), BF16),
        pltpu.VMEM((n_ep * rows, cols), F32),
        pltpu.VMEM((128, 128), F32),
        pltpu.VMEM((n_tp, rows, 128), F32),
        pltpu.SemaphoreType.DMA((12,)),
        pltpu.SemaphoreType.DMA((heads,)),
        pltpu.SemaphoreType.DMA((5 + 2 * n_ep,)),
        pltpu.SemaphoreType.DMA((5 + 2 * n_ep,)),
    ]
    kernel = functools.partial(layer_kernel, n_ep, n_tp)
    row = lambda a: a.reshape(1, -1)
    mixed_out, new_state = pl.pallas_call(
        kernel,
        out_shape=(
            jax.ShapeDtypeStruct(hidden_in.shape, BF16),
            jax.ShapeDtypeStruct(state.shape, F32),
        ),
        in_specs=[vmem] * 9 + [hbm] * 12,
        out_specs=(vmem, hbm),
        scratch_shapes=scratch,
        compiler_params=pltpu.CompilerParams(
            collective_id=0, has_side_effects=True, vmem_limit_bytes=60 * 1024 * 1024
        ),
    )(
        hidden_in,
        lower_bound,
        row(head_gain),
        row(ln1_gain),
        row(ln1_bias),
        routes.T,
        route_weights.T,
        row(ln2_gain),
        row(ln2_bias),
        *whole,
    )
    return (mixed_out, new_state)


def fits(mesh, hidden_in, state, exp_gate):
    n_tp = mesh.shape["tp"]
    n_ep = mesh.shape["ep"]
    seqs = hidden_in.shape[0] // n_ep
    cols = hidden_in.shape[1] // n_tp
    weights = 3 * exp_gate.size * 2 // (n_tp * n_ep) + state.size * 4 // (n_tp * n_ep)
    return (
        cols % 128 == 0
        and seqs <= 16
        and state.shape[2] == 128
        and exp_gate.shape[0] <= 128
        and n_tp * n_ep <= 64
        and weights <= 24 * 1024 * 1024
    )


def rounded(value):
    return lax.optimization_barrier(value.astype(jnp.bfloat16)).astype(jnp.float32)


def local(
    hidden_in,
    state,
    lower_bound,
    w_forget,
    w_input,
    w_query,
    w_outgate,
    head_gain,
    w_out,
    ln1_gain,
    ln1_bias,
    routes,
    route_weights,
    exp_gate,
    exp_up,
    exp_down,
    sh_gate,
    sh_up,
    sh_down,
    ln2_gain,
    ln2_bias,
):
    n_tp = lax.axis_size("tp")
    n_ep = lax.axis_size("ep")
    seq_count = hidden_in.shape[0]
    col_count = hidden_in.shape[1]
    model_width = col_count * n_tp
    col_start = lax.axis_index("tp") * col_count
    heads_dev = state.shape[1]
    head_size = state.shape[2]
    top_count = routes.shape[1]
    local_experts = exp_gate.shape[0]
    expert_count = local_experts * n_ep
    capacity = max(2, 3 * seq_count * top_count // (2 * expert_count))
    slot_count = expert_count * capacity
    rows_full = lax.all_gather(hidden_in, "tp", axis=1, tiled=True)

    def project(weight):
        product = jnp.dot(rows_full, weight, preferred_element_type=jnp.float32)
        return rounded(product).reshape(seq_count, heads_dev, head_size)

    forget_pre = project(w_forget)
    forget = lower_bound + (1.0 - lower_bound) * jax.nn.sigmoid(forget_pre)
    key_part = (1.0 - lower_bound) * jax.nn.sigmoid(-forget_pre)
    values = project(w_input)
    queries = jax.nn.silu(project(w_query))
    out_gate = jax.nn.silu(project(w_outgate))
    new_state = forget[..., None] * state + key_part[..., None] * values[:, :, None, :]
    readout = jnp.einsum("bhd,bhdv->bhv", queries, new_state, precision=lax.Precision.HIGHEST)
    normed = readout * lax.rsqrt(jnp.mean(readout * readout, -1, keepdims=True) + EPS) * head_gain
    mixed = (normed * out_gate).astype(jnp.bfloat16).reshape(seq_count, heads_dev * head_size)
    branch = jnp.dot(mixed, w_out, preferred_element_type=jnp.float32)
    summed = lax.psum(branch.astype(jnp.bfloat16), "tp").astype(jnp.float32)
    residual = ALPHA * rows_full.astype(jnp.float32) + summed
    average = jnp.mean(residual, -1, keepdims=True)
    centered = residual - average
    variance = jnp.mean(centered * centered, -1, keepdims=True)
    normed_rows = (centered * lax.rsqrt(variance + EPS) * ln1_gain + ln1_bias).astype(jnp.bfloat16)
    routes_flat = routes.reshape(-1)
    one_hot = (routes_flat[:, None] == jnp.arange(expert_count, dtype=jnp.int32)[None, :]).astype(
        jnp.int32
    )
    position = jnp.sum((jnp.cumsum(one_hot, 0) - one_hot) * one_hot, 1)
    slot_index = routes_flat * capacity + position
    placing = (slot_index[:, None] == jnp.arange(slot_count, dtype=jnp.int32)[None, :]).astype(
        jnp.float32
    )
    chooser = jnp.sum(placing.reshape(seq_count, top_count, slot_count), 1).astype(jnp.bfloat16)
    weighted = jnp.sum(
        (placing * route_weights.reshape(-1)[:, None]).reshape(seq_count, top_count, slot_count), 1
    )
    own_cols = lax.dynamic_slice_in_dim(normed_rows, col_start, col_count, 1)
    picked = lax.dot_general(
        chooser, normed_rows, (((0,), (0,)), ((), ())), preferred_element_type=jnp.float32
    )
    arrived = lax.all_to_all(
        picked.astype(jnp.bfloat16).reshape(n_ep, local_experts * capacity, normed_rows.shape[1]),
        "ep",
        split_axis=0,
        concat_axis=0,
        tiled=True,
    )
    blocks = arrived.reshape(n_ep, local_experts, capacity, model_width)
    gate_part = jnp.einsum("gecd,edf->gecf", blocks, exp_gate, preferred_element_type=jnp.float32)
    up_part = jnp.einsum("gecd,edf->gecf", blocks, exp_up, preferred_element_type=jnp.float32)
    hidden_part = (jax.nn.silu(gate_part) * up_part).astype(jnp.bfloat16)
    expert_part = jnp.einsum(
        "gecf,efd->gecd", hidden_part, exp_down, preferred_element_type=jnp.float32
    )
    expert_part = expert_part.reshape(n_ep, local_experts * capacity, model_width).astype(
        jnp.bfloat16
    )
    shared_hidden = (
        jax.nn.silu(jnp.dot(normed_rows, sh_gate, preferred_element_type=jnp.float32))
        * jnp.dot(normed_rows, sh_up, preferred_element_type=jnp.float32)
    ).astype(jnp.bfloat16)
    shared_part = jnp.dot(shared_hidden, sh_down, preferred_element_type=jnp.float32)
    returned = lax.all_to_all(expert_part, "ep", split_axis=0, concat_axis=0, tiled=True)
    routed_partial = jnp.dot(
        weighted,
        returned.reshape(slot_count, model_width).astype(jnp.float32),
        precision=lax.Precision.HIGHEST,
    )
    combined = lax.psum_scatter(
        (routed_partial + shared_part).astype(jnp.bfloat16), "tp", scatter_dimension=1, tiled=True
    ).astype(jnp.float32)
    final_in = ALPHA * own_cols.astype(jnp.float32) + combined
    moments_two = lax.psum((jnp.sum(final_in, -1), jnp.sum(final_in * final_in, -1)), "tp")
    average_two = moments_two[0][:, None] / model_width
    variance_two = moments_two[1][:, None] / model_width - average_two * average_two
    gain_two = lax.dynamic_slice_in_dim(ln2_gain, col_start, col_count)
    bias_two = lax.dynamic_slice_in_dim(ln2_bias, col_start, col_count)
    mixed_out = (
        (final_in - average_two) * lax.rsqrt(variance_two + EPS) * gain_two + bias_two
    ).astype(jnp.bfloat16)
    return (mixed_out, new_state)


def solution(mesh):
    placed = (
        P("ep", "tp"),
        P("ep", "tp", None, None),
        P("tp", None),
        P(None, "tp"),
        P(None, "tp"),
        P(None, "tp"),
        P(None, "tp"),
        P(),
        P("tp", None),
        P(),
        P(),
        P("ep", None),
        P("ep", None),
        P("ep", None, "tp"),
        P("ep", None, "tp"),
        P("ep", "tp", None),
        P(None, "tp"),
        P(None, "tp"),
        P("tp", None),
        P(),
        P(),
    )

    def layer(*arrays):
        chosen = fused if fits(mesh, arrays[0], arrays[1], arrays[13]) else local
        return jax.shard_map(
            chosen,
            mesh=mesh,
            in_specs=placed,
            out_specs=(P("ep", "tp"), P("ep", "tp", None, None)),
            check_vma=False,
        )(*arrays)

    return layer
```

```python
import functools

import jax
import jax.numpy as jnp
from jax import lax
from jax.experimental import pallas as pl
from jax.experimental.pallas import tpu as pltpu
from jax.sharding import PartitionSpec as P

EPS = 1e-05
ALPHA = 2.0**0.25
MESH = pl.DeviceIdType.MESH
F32 = jnp.float32
BF16 = jnp.bfloat16


def sigmoid(value):
    return jax.nn.sigmoid(value)


def silu(value):
    return value * jax.nn.sigmoid(value)


def dot(left, right):
    return jnp.dot(left, right, preferred_element_type=F32)


def dot_t(left, right):
    dims = (((1,), (1,)), ((), ()))
    return lax.dot_general(left, right, dims, preferred_element_type=F32)


def layer_kernel(
    n_ep,
    n_tp,
    hid,
    lb,
    hg,
    g1,
    b1,
    routes,
    rw,
    g2,
    b2,
    state_h,
    wf_h,
    wi_h,
    wq_h,
    wo_h,
    wout_h,
    eg_h,
    eu_h,
    ed_h,
    sg_h,
    su_h,
    sd_h,
    out,
    ns,
    st,
    wf,
    wi,
    wq,
    wo,
    wout,
    eg,
    eu,
    ed,
    sg,
    su,
    sd,
    xf,
    xs,
    cws,
    cols_t,
    vals,
    ro,
    rs_send,
    rs,
    res,
    nr,
    cw_col,
    a2a_send,
    a2a,
    z_send,
    z_recv,
    acc_buf,
    cw_t,
    stat,
    load_sem,
    send_sem,
    recv_sem,
):
    me_e = lax.axis_index("ep")
    me_t = lax.axis_index("tp")
    seqs = hid.shape[0]
    cols = hid.shape[1]
    rows = xf.shape[0]
    heads = lb.shape[0]
    head = lb.shape[1]
    local_experts = eg.shape[0]

    first = [(wf_h, wf), (wi_h, wi), (wq_h, wq), (wo_h, wo), (state_h, st), (wout_h, wout)]
    second = [(eg_h, eg), (eu_h, eu), (sg_h, sg), (su_h, su), (ed_h, ed), (sd_h, sd)]
    loads = {}

    def start_loads(pairs, base):
        for i, (src, dst) in enumerate(pairs):
            loads[base + i] = pltpu.make_async_copy(src, dst, load_sem.at[base + i])
            loads[base + i].start()

    barrier = pltpu.get_barrier_semaphore()
    for k in range(1, n_ep):
        target = (lax.rem(me_e + k, n_ep), me_t)
        pl.semaphore_signal(barrier, inc=1, device_id=target, device_id_type=MESH)
    for k in range(1, n_tp):
        target = (me_e, lax.rem(me_t + k, n_tp))
        pl.semaphore_signal(barrier, inc=1, device_id=target, device_id_type=MESH)
    start_loads(first, 0)

    xf[...] = jnp.zeros_like(xf)
    xf[0:seqs, :] = hid[...].astype(F32)
    own_hidden = xf[...]
    xs[me_t] = own_hidden.astype(BF16)
    names = lax.broadcasted_iota(jnp.int32, (cw_t.shape[0], seqs), 0)
    own_cw = jnp.zeros(names.shape, F32)
    for k in range(routes.shape[0]):
        own_cw += jnp.where(names == routes[k : k + 1, :], rw[k : k + 1, :], 0.0)
    cw_t[...] = jnp.zeros_like(cw_t)
    cw_t[:, 0:seqs] = own_cw
    cws[me_e] = cw_t[...].T[0:rows, :]

    pl.semaphore_wait(barrier, n_ep + n_tp - 2)

    sends = []

    def send(src, dst, phase, target):
        copy = pltpu.make_async_remote_copy(
            src_ref=src,
            dst_ref=dst,
            send_sem=send_sem.at[phase],
            recv_sem=recv_sem.at[phase],
            device_id=target,
            device_id_type=MESH,
        )
        copy.start()
        sends.append(copy)

    def arrived(buffer, count, phase):
        part = buffer.at[pl.ds(0, count)]
        pltpu.make_async_copy(part, part, recv_sem.at[phase]).wait()

    for k in range(1, n_tp):
        send(xs.at[me_t], xs.at[me_t], 0, (me_e, lax.rem(me_t + k, n_tp)))
    for k in range(1, n_ep):
        send(cws.at[me_e], cws.at[me_e], 1, (lax.rem(me_e + k, n_ep), me_t))
    start_loads(second, len(first))

    arrived(xs, n_tp - 1, 0)
    x_full = jnp.concatenate([xs[t] for t in range(n_tp)], axis=1)

    def project(weight, index):
        loads[index].wait()
        return dot(x_full, weight[...]).astype(BF16).astype(F32)

    forget_pre = project(wf, 0)
    value_in = project(wi, 1)
    query = silu(project(wq, 2))
    out_gate = silu(project(wo, 3))
    for h in range(heads):
        span = slice(h * head, (h + 1) * head)
        bound = lb[h : h + 1, :]
        pre = forget_pre[:, span]
        forget = bound + (1.0 - bound) * sigmoid(pre)
        key = (1.0 - bound) * sigmoid(-pre)
        stacked = jnp.concatenate(
            [forget, key, query[:, span], jnp.zeros((head - 3 * rows, head), F32)], axis=0
        )
        cols_t[h] = stacked.T
        vals[h] = value_in[:, span]
    loads[4].wait()
    ro[...] = jnp.zeros_like(ro)
    for h in range(heads):
        for b in range(seqs):
            f_col = cols_t[h, :, b : b + 1]
            k_col = cols_t[h, :, rows + b : rows + b + 1]
            q_col = cols_t[h, :, 2 * rows + b : 2 * rows + b + 1]
            new = f_col * st[b, h] + k_col * vals[h, b : b + 1, :]
            ns[b, h] = new
            ro[h, b : b + 1, :] = jnp.sum(q_col * new, axis=0, keepdims=True)
    mixed = []
    for h in range(heads):
        readout = ro[h]
        scale = lax.rsqrt(jnp.mean(readout * readout, -1, keepdims=True) + EPS)
        gate = out_gate[:, h * head : (h + 1) * head]
        mixed.append((readout * scale * hg[...] * gate).astype(BF16))
    mixed = jnp.concatenate(mixed, axis=1)
    loads[5].wait()
    for k in list(range(1, n_tp)) + [0]:
        peer = lax.rem(me_t + k, n_tp)
        block = dot(mixed, wout[:, pl.ds(pl.multiple_of(peer * cols, cols), cols)])
        if k:
            rs_send[peer] = block.astype(BF16)
            send(rs_send.at[peer], rs.at[me_t], 2, (me_e, peer))
        else:
            rs[me_t] = block.astype(BF16)
    arrived(rs, n_tp - 1, 2)
    total = ALPHA * own_hidden
    for t in range(n_tp):
        total += rs[t].astype(F32)
    res[me_e, me_t] = total.astype(BF16)
    near = sorted(range(n_ep), key=lambda k: min(k, n_ep - k))
    for k in reversed(near[1:]):
        piece = res.at[me_e, me_t]
        send(piece, piece, 5 + k, (lax.rem(me_e + k, n_ep), me_t))
    width = n_tp * cols

    def forward(k):
        group = lax.rem(me_e + n_ep - k, n_ep)
        piece = res.at[group, me_t]
        if k:
            pltpu.make_async_copy(piece, piece, recv_sem.at[5 + k]).wait()
        for i in range(1, n_tp):
            send(piece, piece, 5 + n_ep + k, (me_e, lax.rem(me_t + i, n_tp)))

    def norm_group(k):
        group = lax.rem(me_e + n_ep - k, n_ep)
        arrived(res.at[group], n_tp - 1, 5 + n_ep + k)
        row = jnp.concatenate([res[group, t] for t in range(n_tp)], axis=1).astype(F32)
        centered = row - jnp.sum(row, -1, keepdims=True) / width
        variance = jnp.sum(centered * centered, -1, keepdims=True) / width
        normed = centered * lax.rsqrt(variance + EPS) * g1[...] + b1[...]
        nr[pl.ds(pl.multiple_of(group * rows, rows), rows), :] = normed.astype(BF16)

    forward(0)
    arrived(cws, n_ep - 1, 1)
    for g in range(n_ep):
        for j in range(local_experts):
            at = lax.broadcasted_iota(jnp.int32, cws.shape[1:], 1)
            cw_col[j, g * rows : (g + 1) * rows, :] = jnp.sum(
                jnp.where(at == me_e * local_experts + j, cws[g], 0.0), axis=1, keepdims=True
            )
    base = len(first)
    for k in near[1:]:
        forward(k)
    norm_group(0)
    own_rows = nr[pl.ds(pl.multiple_of(me_e * rows, rows), rows), :]
    loads[base + 2].wait()
    loads[base + 3].wait()
    shared = (silu(dot_t(own_rows, sg[...])) * dot_t(own_rows, su[...])).astype(BF16)
    for k in near[1:]:
        norm_group(k)
    all_rows = nr[...]
    loads[base].wait()
    loads[base + 1].wait()
    hidden = []
    for j in range(local_experts):
        hidden.append((silu(dot(all_rows, eg[j])) * dot(all_rows, eu[j])).astype(BF16))
    loads[base + 4].wait()
    loads[base + 5].wait()
    weights = [cw_col[j] for j in range(local_experts)]
    own_span = pl.ds(pl.multiple_of(me_e * rows, rows), rows)
    for k in list(range(1, n_tp)) + [0]:
        peer = lax.rem(me_t + k, n_tp)
        span = pl.ds(pl.multiple_of(peer * cols, cols), cols)
        acc = jnp.zeros((n_ep * rows, cols), F32)
        for j in range(local_experts):
            part = dot(hidden[j], ed[j, :, span]).astype(BF16).astype(F32)
            acc += weights[j] * part
        acc_buf[...] = acc
        acc_buf[own_span, :] += dot(shared, sd[:, span])
        if k:
            a2a_send[peer] = acc_buf[...].astype(BF16)
            send(a2a_send.at[peer], a2a.at[me_t], 4, (me_e, peer))
        else:
            a2a[me_t] = acc_buf[...].astype(BF16)
    start = pl.multiple_of(me_t * cols, cols)
    own_cols = nr[own_span, pl.ds(start, cols)]
    arrived(a2a, n_tp - 1, 4)
    plane = a2a[0].astype(F32)
    for i in range(1, n_tp):
        plane += a2a[i].astype(F32)
    acc_buf[...] = plane
    for g in range(n_ep):
        z_send[g] = plane[g * rows : (g + 1) * rows].astype(BF16)
    for k in range(1, n_ep):
        peer = lax.rem(me_e + k, n_ep)
        send(z_send.at[peer], z_recv.at[me_e], 3, (peer, me_t))
    z_recv[me_e] = z_send[me_e]
    final = ALPHA * own_cols.astype(F32)
    arrived(z_recv, n_ep - 1, 3)
    for g in range(n_ep):
        final += z_recv[g].astype(F32)
    mean_own = jnp.sum(final, -1, keepdims=True) / cols
    apart = final - mean_own
    spread_own = jnp.sum(apart * apart, -1, keepdims=True)
    lane = lax.broadcasted_iota(jnp.int32, stat.shape[1:], 1)
    stat[me_t] = jnp.where(lane == 0, mean_own, spread_own)
    for k in range(1, n_tp):
        send(stat.at[me_t], stat.at[me_t], 5, (me_e, lax.rem(me_t + k, n_tp)))
    gain = g2[:, pl.ds(start, cols)]
    bias = b2[:, pl.ds(start, cols)]
    arrived(stat, n_tp - 1, 5)
    means = [stat[t, :, 0:1] for t in range(n_tp)]
    mean = sum(means) / n_tp
    spread = jnp.zeros_like(mean)
    for t in range(n_tp):
        spread += stat[t, :, 1:2] + cols * (means[t] - mean) * (means[t] - mean)
    result = (final - mean) * lax.rsqrt(spread / width + EPS) * gain + bias
    out[...] = result[0:seqs, :].astype(BF16)
    for copy in sends:
        copy.wait_send()


def fused(
    hidden_in,
    state,
    lower_bound,
    w_forget,
    w_input,
    w_query,
    w_outgate,
    head_gain,
    w_out,
    ln1_gain,
    ln1_bias,
    routes,
    route_weights,
    exp_gate,
    exp_up,
    exp_down,
    sh_gate,
    sh_up,
    sh_down,
    ln2_gain,
    ln2_bias,
):
    n_tp = lax.axis_size("tp")
    n_ep = lax.axis_size("ep")
    seqs, cols = hidden_in.shape
    rows = -(-seqs // 16) * 16
    heads, head = lower_bound.shape
    local_experts = exp_gate.shape[0]
    whole = [
        state,
        w_forget,
        w_input,
        w_query,
        w_outgate,
        w_out,
        exp_gate,
        exp_up,
        exp_down,
        sh_gate.T,
        sh_up.T,
        sh_down,
    ]
    vmem = pl.BlockSpec(memory_space=pltpu.VMEM)
    hbm = pl.BlockSpec(memory_space=pltpu.HBM)
    scratch = [pltpu.VMEM(a.shape, a.dtype) for a in whole]
    scratch += [
        pltpu.VMEM((rows, cols), F32),
        pltpu.VMEM((n_tp, rows, cols), BF16),
        pltpu.VMEM((n_ep, rows, 128), F32),
        pltpu.VMEM((heads, head, head), F32),
        pltpu.VMEM((heads, rows, head), F32),
        pltpu.VMEM((heads, rows, head), F32),
        pltpu.VMEM((n_tp, rows, cols), BF16),
        pltpu.VMEM((n_tp, rows, cols), BF16),
        pltpu.VMEM((n_ep, n_tp, rows, cols), BF16),
        pltpu.VMEM((n_ep * rows, n_tp * cols), BF16),
        pltpu.VMEM((local_experts, n_ep * rows, 1), F32),
        pltpu.VMEM((n_tp, n_ep * rows, cols), BF16),
        pltpu.VMEM((n_tp, n_ep * rows, cols), BF16),
        pltpu.VMEM((n_ep, rows, cols), BF16),
        pltpu.VMEM((n_ep, rows, cols), BF16),
        pltpu.VMEM((n_ep * rows, cols), F32),
        pltpu.VMEM((128, 128), F32),
        pltpu.VMEM((n_tp, rows, 128), F32),
        pltpu.SemaphoreType.DMA((12,)),
        pltpu.SemaphoreType.DMA((5 + 2 * n_ep,)),
        pltpu.SemaphoreType.DMA((5 + 2 * n_ep,)),
    ]
    kernel = functools.partial(layer_kernel, n_ep, n_tp)
    row = lambda a: a.reshape(1, -1)
    mixed_out, new_state = pl.pallas_call(
        kernel,
        out_shape=(
            jax.ShapeDtypeStruct(hidden_in.shape, BF16),
            pltpu.VMEM(state.shape, F32),
        ),
        in_specs=[vmem] * 9 + [hbm] * 12,
        out_specs=(vmem, vmem),
        scratch_shapes=scratch,
        compiler_params=pltpu.CompilerParams(
            collective_id=0, has_side_effects=True, vmem_limit_bytes=63_400_000
        ),
    )(
        hidden_in,
        lower_bound,
        row(head_gain),
        row(ln1_gain),
        row(ln1_bias),
        routes.T,
        route_weights.T,
        row(ln2_gain),
        row(ln2_bias),
        *whole,
    )
    return (mixed_out, new_state)


def fits(mesh, hidden_in, state, exp_gate):
    n_tp = mesh.shape["tp"]
    n_ep = mesh.shape["ep"]
    seqs = hidden_in.shape[0] // n_ep
    cols = hidden_in.shape[1] // n_tp
    weights = 3 * exp_gate.size * 2 // (n_tp * n_ep) + state.size * 4 // (n_tp * n_ep)
    return (
        cols % 128 == 0
        and seqs <= 16
        and state.shape[2] == 128
        and exp_gate.shape[0] <= 128
        and n_tp * n_ep <= 64
        and weights <= 24 * 1024 * 1024
    )


def rounded(value):
    return lax.optimization_barrier(value.astype(jnp.bfloat16)).astype(jnp.float32)


def local(
    hidden_in,
    state,
    lower_bound,
    w_forget,
    w_input,
    w_query,
    w_outgate,
    head_gain,
    w_out,
    ln1_gain,
    ln1_bias,
    routes,
    route_weights,
    exp_gate,
    exp_up,
    exp_down,
    sh_gate,
    sh_up,
    sh_down,
    ln2_gain,
    ln2_bias,
):
    n_tp = lax.axis_size("tp")
    n_ep = lax.axis_size("ep")
    seq_count = hidden_in.shape[0]
    col_count = hidden_in.shape[1]
    model_width = col_count * n_tp
    col_start = lax.axis_index("tp") * col_count
    heads_dev = state.shape[1]
    head_size = state.shape[2]
    top_count = routes.shape[1]
    local_experts = exp_gate.shape[0]
    expert_count = local_experts * n_ep
    capacity = max(2, 3 * seq_count * top_count // (2 * expert_count))
    slot_count = expert_count * capacity
    rows_full = lax.all_gather(hidden_in, "tp", axis=1, tiled=True)

    def project(weight):
        product = jnp.dot(rows_full, weight, preferred_element_type=jnp.float32)
        return rounded(product).reshape(seq_count, heads_dev, head_size)

    forget_pre = project(w_forget)
    forget = lower_bound + (1.0 - lower_bound) * jax.nn.sigmoid(forget_pre)
    key_part = (1.0 - lower_bound) * jax.nn.sigmoid(-forget_pre)
    values = project(w_input)
    queries = jax.nn.silu(project(w_query))
    out_gate = jax.nn.silu(project(w_outgate))
    new_state = forget[..., None] * state + key_part[..., None] * values[:, :, None, :]
    readout = jnp.einsum("bhd,bhdv->bhv", queries, new_state, precision=lax.Precision.HIGHEST)
    normed = readout * lax.rsqrt(jnp.mean(readout * readout, -1, keepdims=True) + EPS) * head_gain
    mixed = (normed * out_gate).astype(jnp.bfloat16).reshape(seq_count, heads_dev * head_size)
    branch = jnp.dot(mixed, w_out, preferred_element_type=jnp.float32)
    summed = lax.psum(branch.astype(jnp.bfloat16), "tp").astype(jnp.float32)
    residual = ALPHA * rows_full.astype(jnp.float32) + summed
    average = jnp.mean(residual, -1, keepdims=True)
    centered = residual - average
    variance = jnp.mean(centered * centered, -1, keepdims=True)
    normed_rows = (centered * lax.rsqrt(variance + EPS) * ln1_gain + ln1_bias).astype(jnp.bfloat16)
    routes_flat = routes.reshape(-1)
    one_hot = (routes_flat[:, None] == jnp.arange(expert_count, dtype=jnp.int32)[None, :]).astype(
        jnp.int32
    )
    position = jnp.sum((jnp.cumsum(one_hot, 0) - one_hot) * one_hot, 1)
    slot_index = routes_flat * capacity + position
    placing = (slot_index[:, None] == jnp.arange(slot_count, dtype=jnp.int32)[None, :]).astype(
        jnp.float32
    )
    chooser = jnp.sum(placing.reshape(seq_count, top_count, slot_count), 1).astype(jnp.bfloat16)
    weighted = jnp.sum(
        (placing * route_weights.reshape(-1)[:, None]).reshape(seq_count, top_count, slot_count), 1
    )
    own_cols = lax.dynamic_slice_in_dim(normed_rows, col_start, col_count, 1)
    picked = lax.dot_general(
        chooser, normed_rows, (((0,), (0,)), ((), ())), preferred_element_type=jnp.float32
    )
    arrived = lax.all_to_all(
        picked.astype(jnp.bfloat16).reshape(n_ep, local_experts * capacity, normed_rows.shape[1]),
        "ep",
        split_axis=0,
        concat_axis=0,
        tiled=True,
    )
    blocks = arrived.reshape(n_ep, local_experts, capacity, model_width)
    gate_part = jnp.einsum("gecd,edf->gecf", blocks, exp_gate, preferred_element_type=jnp.float32)
    up_part = jnp.einsum("gecd,edf->gecf", blocks, exp_up, preferred_element_type=jnp.float32)
    hidden_part = (jax.nn.silu(gate_part) * up_part).astype(jnp.bfloat16)
    expert_part = jnp.einsum(
        "gecf,efd->gecd", hidden_part, exp_down, preferred_element_type=jnp.float32
    )
    expert_part = expert_part.reshape(n_ep, local_experts * capacity, model_width).astype(
        jnp.bfloat16
    )
    shared_hidden = (
        jax.nn.silu(jnp.dot(normed_rows, sh_gate, preferred_element_type=jnp.float32))
        * jnp.dot(normed_rows, sh_up, preferred_element_type=jnp.float32)
    ).astype(jnp.bfloat16)
    shared_part = jnp.dot(shared_hidden, sh_down, preferred_element_type=jnp.float32)
    returned = lax.all_to_all(expert_part, "ep", split_axis=0, concat_axis=0, tiled=True)
    routed_partial = jnp.dot(
        weighted,
        returned.reshape(slot_count, model_width).astype(jnp.float32),
        precision=lax.Precision.HIGHEST,
    )
    combined = lax.psum_scatter(
        (routed_partial + shared_part).astype(jnp.bfloat16), "tp", scatter_dimension=1, tiled=True
    ).astype(jnp.float32)
    final_in = ALPHA * own_cols.astype(jnp.float32) + combined
    moments_two = lax.psum((jnp.sum(final_in, -1), jnp.sum(final_in * final_in, -1)), "tp")
    average_two = moments_two[0][:, None] / model_width
    variance_two = moments_two[1][:, None] / model_width - average_two * average_two
    gain_two = lax.dynamic_slice_in_dim(ln2_gain, col_start, col_count)
    bias_two = lax.dynamic_slice_in_dim(ln2_bias, col_start, col_count)
    mixed_out = (
        (final_in - average_two) * lax.rsqrt(variance_two + EPS) * gain_two + bias_two
    ).astype(jnp.bfloat16)
    return (mixed_out, new_state)


def solution(mesh):
    placed = (
        P("ep", "tp"),
        P("ep", "tp", None, None),
        P("tp", None),
        P(None, "tp"),
        P(None, "tp"),
        P(None, "tp"),
        P(None, "tp"),
        P(),
        P("tp", None),
        P(),
        P(),
        P("ep", None),
        P("ep", None),
        P("ep", None, "tp"),
        P("ep", None, "tp"),
        P("ep", "tp", None),
        P(None, "tp"),
        P(None, "tp"),
        P("tp", None),
        P(),
        P(),
    )

    def layer(*arrays):
        chosen = fused if fits(mesh, arrays[0], arrays[1], arrays[13]) else local
        return jax.shard_map(
            chosen,
            mesh=mesh,
            in_specs=placed,
            out_specs=(P("ep", "tp"), P("ep", "tp", None, None)),
            check_vma=False,
        )(*arrays)

    return layer
```

```python
import functools

import jax
import jax.numpy as jnp
from jax import lax
from jax.experimental import pallas as pl
from jax.experimental.pallas import tpu as pltpu
from jax.sharding import PartitionSpec as P

EPS = 1e-05
ALPHA = 2.0**0.25
MESH = pl.DeviceIdType.MESH
F32 = jnp.float32
BF16 = jnp.bfloat16


def sigmoid(value):
    return jax.nn.sigmoid(value)


def silu(value):
    return value * jax.nn.sigmoid(value)


def dot(left, right):
    return jnp.dot(left, right, preferred_element_type=F32)


def dot_t(left, right):
    dims = (((1,), (1,)), ((), ()))
    return lax.dot_general(left, right, dims, preferred_element_type=F32)


def layer_kernel(
    n_ep,
    n_tp,
    hid,
    lb,
    hg,
    g1,
    b1,
    routes,
    rw,
    g2,
    b2,
    state_h,
    wf_h,
    wi_h,
    wq_h,
    wo_h,
    wout_h,
    eg_h,
    eu_h,
    ed_h,
    sg_h,
    su_h,
    sd_h,
    out,
    ns,
    st,
    wf,
    wi,
    wq,
    wo,
    wout,
    eg,
    eu,
    ed,
    sg,
    su,
    sd,
    xf,
    xs,
    cws,
    cols_t,
    vals,
    ro,
    rs_send,
    rs,
    res,
    nr,
    cw_col,
    a2a_send,
    a2a,
    z_send,
    z_recv,
    acc_buf,
    cw_t,
    stat,
    load_sem,
    send_sem,
    recv_sem,
):
    me_e = lax.axis_index("ep")
    me_t = lax.axis_index("tp")
    seqs = hid.shape[0]
    cols = hid.shape[1]
    rows = xf.shape[0]
    heads = lb.shape[0]
    head = lb.shape[1]
    local_experts = eg.shape[0]

    first = [(wf_h, wf), (wi_h, wi), (wq_h, wq), (wo_h, wo), (state_h, st), (wout_h, wout)]
    second = [(eg_h, eg), (eu_h, eu), (sg_h, sg), (su_h, su), (ed_h, ed), (sd_h, sd)]
    loads = {}

    def start_loads(pairs, base):
        for i, (src, dst) in enumerate(pairs):
            loads[base + i] = pltpu.make_async_copy(src, dst, load_sem.at[base + i])
            loads[base + i].start()

    barrier = pltpu.get_barrier_semaphore()
    for k in range(1, n_ep):
        target = (lax.rem(me_e + k, n_ep), me_t)
        pl.semaphore_signal(barrier, inc=1, device_id=target, device_id_type=MESH)
    for k in range(1, n_tp):
        target = (me_e, lax.rem(me_t + k, n_tp))
        pl.semaphore_signal(barrier, inc=1, device_id=target, device_id_type=MESH)
    start_loads(first, 0)

    xf[...] = jnp.zeros_like(xf)
    xf[0:seqs, :] = hid[...].astype(F32)
    own_hidden = xf[...]
    xs[me_t] = own_hidden.astype(BF16)
    names = lax.broadcasted_iota(jnp.int32, (cw_t.shape[0], seqs), 0)
    own_cw = jnp.zeros(names.shape, F32)
    for k in range(routes.shape[0]):
        own_cw += jnp.where(names == routes[k : k + 1, :], rw[k : k + 1, :], 0.0)
    cw_t[...] = jnp.zeros_like(cw_t)
    cw_t[:, 0:seqs] = own_cw
    cws[me_e] = cw_t[...].T[0:rows, :]

    pl.semaphore_wait(barrier, n_ep + n_tp - 2)

    sends = []

    def send(src, dst, phase, target):
        copy = pltpu.make_async_remote_copy(
            src_ref=src,
            dst_ref=dst,
            send_sem=send_sem.at[phase],
            recv_sem=recv_sem.at[phase],
            device_id=target,
            device_id_type=MESH,
        )
        copy.start()
        sends.append(copy)

    def arrived(buffer, count, phase):
        part = buffer.at[pl.ds(0, count)]
        pltpu.make_async_copy(part, part, recv_sem.at[phase]).wait()

    for k in range(1, n_tp):
        send(xs.at[me_t], xs.at[me_t], 0, (me_e, lax.rem(me_t + k, n_tp)))
    for k in range(1, n_ep):
        send(cws.at[me_e], cws.at[me_e], 1, (lax.rem(me_e + k, n_ep), me_t))
    start_loads(second, len(first))

    arrived(xs, n_tp - 1, 0)
    x_full = jnp.concatenate([xs[t] for t in range(n_tp)], axis=1)

    def project(weight, index):
        loads[index].wait()
        return dot(x_full, weight[...]).astype(BF16).astype(F32)

    forget_pre = project(wf, 0)
    value_in = project(wi, 1)
    query = silu(project(wq, 2))
    out_gate = silu(project(wo, 3))
    for h in range(heads):
        span = slice(h * head, (h + 1) * head)
        bound = lb[h : h + 1, :]
        pre = forget_pre[:, span]
        forget = bound + (1.0 - bound) * sigmoid(pre)
        key = (1.0 - bound) * sigmoid(-pre)
        stacked = jnp.concatenate(
            [forget, key, query[:, span], jnp.zeros((head - 3 * rows, head), F32)], axis=0
        )
        cols_t[h] = stacked.T
        vals[h] = value_in[:, span]
    loads[4].wait()
    ro[...] = jnp.zeros_like(ro)
    for h in range(heads):
        for b in range(seqs):
            f_col = cols_t[h, :, b : b + 1]
            k_col = cols_t[h, :, rows + b : rows + b + 1]
            q_col = cols_t[h, :, 2 * rows + b : 2 * rows + b + 1]
            new = f_col * st[b, h] + k_col * vals[h, b : b + 1, :]
            ns[b, h] = new
            ro[h, b : b + 1, :] = jnp.sum(q_col * new, axis=0, keepdims=True)
    mixed = []
    for h in range(heads):
        readout = ro[h]
        scale = lax.rsqrt(jnp.mean(readout * readout, -1, keepdims=True) + EPS)
        gate = out_gate[:, h * head : (h + 1) * head]
        mixed.append((readout * scale * hg[...] * gate).astype(BF16))
    mixed = jnp.concatenate(mixed, axis=1)
    loads[5].wait()
    for k in list(range(1, n_tp)) + [0]:
        peer = lax.rem(me_t + k, n_tp)
        block = dot(mixed, wout[:, pl.ds(pl.multiple_of(peer * cols, cols), cols)])
        if k:
            rs_send[peer] = block.astype(BF16)
            send(rs_send.at[peer], rs.at[me_t], 2, (me_e, peer))
        else:
            rs[me_t] = block.astype(BF16)
    arrived(rs, n_tp - 1, 2)
    total = ALPHA * own_hidden
    for t in range(n_tp):
        total += rs[t].astype(F32)
    res[me_e, me_t] = total.astype(BF16)
    near = sorted(range(n_ep), key=lambda k: min(k, n_ep - k))
    for k in reversed(near[1:]):
        piece = res.at[me_e, me_t]
        send(piece, piece, 5 + k, (lax.rem(me_e + k, n_ep), me_t))
    width = n_tp * cols

    def forward(k):
        group = lax.rem(me_e + n_ep - k, n_ep)
        piece = res.at[group, me_t]
        if k:
            pltpu.make_async_copy(piece, piece, recv_sem.at[5 + k]).wait()
        for i in range(1, n_tp):
            send(piece, piece, 5 + n_ep + k, (me_e, lax.rem(me_t + i, n_tp)))

    def norm_group(k):
        group = lax.rem(me_e + n_ep - k, n_ep)
        arrived(res.at[group], n_tp - 1, 5 + n_ep + k)
        row = jnp.concatenate([res[group, t] for t in range(n_tp)], axis=1).astype(F32)
        centered = row - jnp.sum(row, -1, keepdims=True) / width
        variance = jnp.sum(centered * centered, -1, keepdims=True) / width
        normed = centered * lax.rsqrt(variance + EPS) * g1[...] + b1[...]
        return normed[0:seqs]

    forward(0)
    arrived(cws, n_ep - 1, 1)
    for k in range(n_ep):
        table = cws[lax.rem(me_e + n_ep - k, n_ep)]
        at = lax.broadcasted_iota(jnp.int32, table.shape, 1)
        for j in range(local_experts):
            column = jnp.where(at == me_e * local_experts + j, table, 0.0)
            cw_col[j, k * seqs : (k + 1) * seqs, :] = jnp.sum(
                column[0:seqs], axis=1, keepdims=True
            )
    base = len(first)
    for k in near[1:]:
        forward(k)
    own_normed = norm_group(0)
    nr[0:seqs, :] = own_normed
    nr[seqs:rows, :] = jnp.zeros((rows - seqs, width), F32)
    own_rows = nr[0:rows, :].astype(BF16)
    loads[base + 2].wait()
    loads[base + 3].wait()
    shared = (silu(dot_t(own_rows, sg[...])) * dot_t(own_rows, su[...])).astype(BF16)
    for k in near[1:]:
        nr[k * seqs : (k + 1) * seqs, :] = norm_group(k)
    all_rows = nr[...].astype(BF16)
    loads[base].wait()
    loads[base + 1].wait()
    hidden = []
    for j in range(local_experts):
        hidden.append((silu(dot(all_rows, eg[j])) * dot(all_rows, eu[j])).astype(BF16))
    loads[base + 4].wait()
    loads[base + 5].wait()
    weights = [cw_col[j] for j in range(local_experts)]
    for k in list(range(1, n_tp)) + [0]:
        peer = lax.rem(me_t + k, n_tp)
        span = pl.ds(pl.multiple_of(peer * cols, cols), cols)
        acc = jnp.zeros(acc_buf.shape, F32)
        for j in range(local_experts):
            part = dot(hidden[j], ed[j, :, span]).astype(BF16).astype(F32)
            acc += weights[j] * part
        acc_buf[...] = acc
        acc_buf[0:seqs, :] += dot(shared, sd[:, span])[0:seqs]
        if k:
            a2a_send[peer] = acc_buf[...].astype(BF16)
            send(a2a_send.at[peer], a2a.at[me_t], 4, (me_e, peer))
        else:
            a2a[me_t] = acc_buf[...].astype(BF16)
    start = pl.multiple_of(me_t * cols, cols)
    xf[0:seqs, :] = nr[0:seqs, pl.ds(start, cols)]
    own_cols = xf[...].astype(BF16)
    arrived(a2a, n_tp - 1, 4)
    plane = a2a[0].astype(F32)
    for i in range(1, n_tp):
        plane += a2a[i].astype(F32)
    for k in reversed(near[1:]):
        xf[0:seqs, :] = plane[k * seqs : (k + 1) * seqs]
        z_send[k] = xf[...].astype(BF16)
        peer = lax.rem(me_e + n_ep - k, n_ep)
        send(z_send.at[k], z_recv.at[me_e], 3, (peer, me_t))
    xf[0:seqs, :] = plane[0:seqs]
    z_recv[me_e] = xf[...].astype(BF16)
    final = ALPHA * own_cols.astype(F32)
    arrived(z_recv, n_ep - 1, 3)
    for g in range(n_ep):
        final += z_recv[g].astype(F32)
    mean_own = jnp.sum(final, -1, keepdims=True) / cols
    apart = final - mean_own
    spread_own = jnp.sum(apart * apart, -1, keepdims=True)
    lane = lax.broadcasted_iota(jnp.int32, stat.shape[1:], 1)
    stat[me_t] = jnp.where(lane == 0, mean_own, spread_own)
    for k in range(1, n_tp):
        send(stat.at[me_t], stat.at[me_t], 5, (me_e, lax.rem(me_t + k, n_tp)))
    gain = g2[:, pl.ds(start, cols)]
    bias = b2[:, pl.ds(start, cols)]
    arrived(stat, n_tp - 1, 5)
    means = [stat[t, :, 0:1] for t in range(n_tp)]
    mean = sum(means) / n_tp
    spread = jnp.zeros_like(mean)
    for t in range(n_tp):
        spread += stat[t, :, 1:2] + cols * (means[t] - mean) * (means[t] - mean)
    result = (final - mean) * lax.rsqrt(spread / width + EPS) * gain + bias
    out[...] = result[0:seqs, :].astype(BF16)
    for copy in sends:
        copy.wait_send()


def fused(
    hidden_in,
    state,
    lower_bound,
    w_forget,
    w_input,
    w_query,
    w_outgate,
    head_gain,
    w_out,
    ln1_gain,
    ln1_bias,
    routes,
    route_weights,
    exp_gate,
    exp_up,
    exp_down,
    sh_gate,
    sh_up,
    sh_down,
    ln2_gain,
    ln2_bias,
):
    n_tp = lax.axis_size("tp")
    n_ep = lax.axis_size("ep")
    seqs, cols = hidden_in.shape
    rows = -(-seqs // 16) * 16
    heads, head = lower_bound.shape
    local_experts = exp_gate.shape[0]
    whole = [
        state,
        w_forget,
        w_input,
        w_query,
        w_outgate,
        w_out,
        exp_gate,
        exp_up,
        exp_down,
        sh_gate.T,
        sh_up.T,
        sh_down,
    ]
    vmem = pl.BlockSpec(memory_space=pltpu.VMEM)
    hbm = pl.BlockSpec(memory_space=pltpu.HBM)
    scratch = [pltpu.VMEM(a.shape, a.dtype) for a in whole]
    scratch += [
        pltpu.VMEM((rows, cols), F32),
        pltpu.VMEM((n_tp, rows, cols), BF16),
        pltpu.VMEM((n_ep, rows, 128), F32),
        pltpu.VMEM((heads, head, head), F32),
        pltpu.VMEM((heads, rows, head), F32),
        pltpu.VMEM((heads, rows, head), F32),
        pltpu.VMEM((n_tp, rows, cols), BF16),
        pltpu.VMEM((n_tp, rows, cols), BF16),
        pltpu.VMEM((n_ep, n_tp, rows, cols), BF16),
        pltpu.VMEM((n_ep * seqs, n_tp * cols), F32),
        pltpu.VMEM((local_experts, n_ep * seqs, 1), F32),
        pltpu.VMEM((n_tp, n_ep * seqs, cols), BF16),
        pltpu.VMEM((n_tp, n_ep * seqs, cols), BF16),
        pltpu.VMEM((n_ep, rows, cols), BF16),
        pltpu.VMEM((n_ep, rows, cols), BF16),
        pltpu.VMEM((n_ep * seqs, cols), F32),
        pltpu.VMEM((128, 128), F32),
        pltpu.VMEM((n_tp, rows, 128), F32),
        pltpu.SemaphoreType.DMA((12,)),
        pltpu.SemaphoreType.DMA((5 + 2 * n_ep,)),
        pltpu.SemaphoreType.DMA((5 + 2 * n_ep,)),
    ]
    kernel = functools.partial(layer_kernel, n_ep, n_tp)
    row = lambda a: a.reshape(1, -1)
    mixed_out, new_state = pl.pallas_call(
        kernel,
        out_shape=(
            jax.ShapeDtypeStruct(hidden_in.shape, BF16),
            pltpu.VMEM(state.shape, F32),
        ),
        in_specs=[vmem] * 9 + [hbm] * 12,
        out_specs=(vmem, vmem),
        scratch_shapes=scratch,
        compiler_params=pltpu.CompilerParams(
            collective_id=0, has_side_effects=True, vmem_limit_bytes=63_400_000
        ),
    )(
        hidden_in,
        lower_bound,
        row(head_gain),
        row(ln1_gain),
        row(ln1_bias),
        routes.T,
        route_weights.T,
        row(ln2_gain),
        row(ln2_bias),
        *whole,
    )
    return (mixed_out, new_state)


def fits(mesh, hidden_in, state, exp_gate):
    n_tp = mesh.shape["tp"]
    n_ep = mesh.shape["ep"]
    seqs = hidden_in.shape[0] // n_ep
    cols = hidden_in.shape[1] // n_tp
    weights = 3 * exp_gate.size * 2 // (n_tp * n_ep) + state.size * 4 // (n_tp * n_ep)
    return (
        cols % 128 == 0
        and seqs <= 16
        and n_ep * seqs % 16 == 0
        and state.shape[2] == 128
        and exp_gate.shape[0] <= 128
        and n_tp * n_ep <= 64
        and weights <= 24 * 1024 * 1024
    )


def rounded(value):
    return lax.optimization_barrier(value.astype(jnp.bfloat16)).astype(jnp.float32)


def local(
    hidden_in,
    state,
    lower_bound,
    w_forget,
    w_input,
    w_query,
    w_outgate,
    head_gain,
    w_out,
    ln1_gain,
    ln1_bias,
    routes,
    route_weights,
    exp_gate,
    exp_up,
    exp_down,
    sh_gate,
    sh_up,
    sh_down,
    ln2_gain,
    ln2_bias,
):
    n_tp = lax.axis_size("tp")
    n_ep = lax.axis_size("ep")
    seq_count = hidden_in.shape[0]
    col_count = hidden_in.shape[1]
    model_width = col_count * n_tp
    col_start = lax.axis_index("tp") * col_count
    heads_dev = state.shape[1]
    head_size = state.shape[2]
    top_count = routes.shape[1]
    local_experts = exp_gate.shape[0]
    expert_count = local_experts * n_ep
    capacity = max(2, 3 * seq_count * top_count // (2 * expert_count))
    slot_count = expert_count * capacity
    rows_full = lax.all_gather(hidden_in, "tp", axis=1, tiled=True)

    def project(weight):
        product = jnp.dot(rows_full, weight, preferred_element_type=jnp.float32)
        return rounded(product).reshape(seq_count, heads_dev, head_size)

    forget_pre = project(w_forget)
    forget = lower_bound + (1.0 - lower_bound) * jax.nn.sigmoid(forget_pre)
    key_part = (1.0 - lower_bound) * jax.nn.sigmoid(-forget_pre)
    values = project(w_input)
    queries = jax.nn.silu(project(w_query))
    out_gate = jax.nn.silu(project(w_outgate))
    new_state = forget[..., None] * state + key_part[..., None] * values[:, :, None, :]
    readout = jnp.einsum("bhd,bhdv->bhv", queries, new_state, precision=lax.Precision.HIGHEST)
    normed = readout * lax.rsqrt(jnp.mean(readout * readout, -1, keepdims=True) + EPS) * head_gain
    mixed = (normed * out_gate).astype(jnp.bfloat16).reshape(seq_count, heads_dev * head_size)
    branch = jnp.dot(mixed, w_out, preferred_element_type=jnp.float32)
    summed = lax.psum(branch.astype(jnp.bfloat16), "tp").astype(jnp.float32)
    residual = ALPHA * rows_full.astype(jnp.float32) + summed
    average = jnp.mean(residual, -1, keepdims=True)
    centered = residual - average
    variance = jnp.mean(centered * centered, -1, keepdims=True)
    normed_rows = (centered * lax.rsqrt(variance + EPS) * ln1_gain + ln1_bias).astype(jnp.bfloat16)
    routes_flat = routes.reshape(-1)
    one_hot = (routes_flat[:, None] == jnp.arange(expert_count, dtype=jnp.int32)[None, :]).astype(
        jnp.int32
    )
    position = jnp.sum((jnp.cumsum(one_hot, 0) - one_hot) * one_hot, 1)
    slot_index = routes_flat * capacity + position
    placing = (slot_index[:, None] == jnp.arange(slot_count, dtype=jnp.int32)[None, :]).astype(
        jnp.float32
    )
    chooser = jnp.sum(placing.reshape(seq_count, top_count, slot_count), 1).astype(jnp.bfloat16)
    weighted = jnp.sum(
        (placing * route_weights.reshape(-1)[:, None]).reshape(seq_count, top_count, slot_count), 1
    )
    own_cols = lax.dynamic_slice_in_dim(normed_rows, col_start, col_count, 1)
    picked = lax.dot_general(
        chooser, normed_rows, (((0,), (0,)), ((), ())), preferred_element_type=jnp.float32
    )
    arrived = lax.all_to_all(
        picked.astype(jnp.bfloat16).reshape(n_ep, local_experts * capacity, normed_rows.shape[1]),
        "ep",
        split_axis=0,
        concat_axis=0,
        tiled=True,
    )
    blocks = arrived.reshape(n_ep, local_experts, capacity, model_width)
    gate_part = jnp.einsum("gecd,edf->gecf", blocks, exp_gate, preferred_element_type=jnp.float32)
    up_part = jnp.einsum("gecd,edf->gecf", blocks, exp_up, preferred_element_type=jnp.float32)
    hidden_part = (jax.nn.silu(gate_part) * up_part).astype(jnp.bfloat16)
    expert_part = jnp.einsum(
        "gecf,efd->gecd", hidden_part, exp_down, preferred_element_type=jnp.float32
    )
    expert_part = expert_part.reshape(n_ep, local_experts * capacity, model_width).astype(
        jnp.bfloat16
    )
    shared_hidden = (
        jax.nn.silu(jnp.dot(normed_rows, sh_gate, preferred_element_type=jnp.float32))
        * jnp.dot(normed_rows, sh_up, preferred_element_type=jnp.float32)
    ).astype(jnp.bfloat16)
    shared_part = jnp.dot(shared_hidden, sh_down, preferred_element_type=jnp.float32)
    returned = lax.all_to_all(expert_part, "ep", split_axis=0, concat_axis=0, tiled=True)
    routed_partial = jnp.dot(
        weighted,
        returned.reshape(slot_count, model_width).astype(jnp.float32),
        precision=lax.Precision.HIGHEST,
    )
    combined = lax.psum_scatter(
        (routed_partial + shared_part).astype(jnp.bfloat16), "tp", scatter_dimension=1, tiled=True
    ).astype(jnp.float32)
    final_in = ALPHA * own_cols.astype(jnp.float32) + combined
    moments_two = lax.psum((jnp.sum(final_in, -1), jnp.sum(final_in * final_in, -1)), "tp")
    average_two = moments_two[0][:, None] / model_width
    variance_two = moments_two[1][:, None] / model_width - average_two * average_two
    gain_two = lax.dynamic_slice_in_dim(ln2_gain, col_start, col_count)
    bias_two = lax.dynamic_slice_in_dim(ln2_bias, col_start, col_count)
    mixed_out = (
        (final_in - average_two) * lax.rsqrt(variance_two + EPS) * gain_two + bias_two
    ).astype(jnp.bfloat16)
    return (mixed_out, new_state)


def solution(mesh):
    placed = (
        P("ep", "tp"),
        P("ep", "tp", None, None),
        P("tp", None),
        P(None, "tp"),
        P(None, "tp"),
        P(None, "tp"),
        P(None, "tp"),
        P(),
        P("tp", None),
        P(),
        P(),
        P("ep", None),
        P("ep", None),
        P("ep", None, "tp"),
        P("ep", None, "tp"),
        P("ep", "tp", None),
        P(None, "tp"),
        P(None, "tp"),
        P("tp", None),
        P(),
        P(),
    )

    def layer(*arrays):
        chosen = fused if fits(mesh, arrays[0], arrays[1], arrays[13]) else local
        return jax.shard_map(
            chosen,
            mesh=mesh,
            in_specs=placed,
            out_specs=(P("ep", "tp"), P("ep", "tp", None, None)),
            check_vma=False,
        )(*arrays)

    return layer
```
